256 devices in a mesh: sp: 64 (over z, x, core), tp: 4 (over y).
Axes of the slice: x: 4, y: 4, z: 8, core: 2. Of those that a mesh axis runs over, the one named last changes fastest.
Arguments:
- x_in: bfloat16 [32768, 1024], P('sp', 'tp'), may hold values from -6 to 6
- gate_b: bfloat16 [32768, 1024], P('sp', 'tp'), may hold values from -6 to 6
- gate_c: bfloat16 [32768, 1024], P('sp', 'tp'), may hold values from -6 to 6
- conv_taps: bfloat16 [3, 1024], P(None, 'tp'), may hold values from -3.5 to 3.5
- out_proj: bfloat16 [1024, 2048], P('tp'), may hold values from -0.1875 to 0.1875
- mix_gain: bfloat16 [2048], replicated, may hold values from 0.099609375 to 1.8984375
- resid: bfloat16 [32768, 2048], P(('sp', 'tp')), may hold values from -6 to 6
- pre_gain: bfloat16 [2048], replicated, may hold values from 0.099609375 to 1.8984375
- expert_gate: bfloat16 [64, 2048, 512], P('sp'), may hold values from -0.125 to 0.125
- expert_up: bfloat16 [64, 2048, 512], P('sp'), may hold values from -0.125 to 0.125
- expert_down: bfloat16 [64, 512, 2048], P('sp'), may hold values from -7.1594562 to 7.1594562
- shared_gate: bfloat16 [2048, 256], replicated, may hold values from -0.125 to 0.125
- shared_up: bfloat16 [2048, 256], replicated, may hold values from -0.125 to 0.125
- shared_down: bfloat16 [256, 2048], replicated, may hold values from -10.125 to 10.125
- post_gain: bfloat16 [2048], replicated, may hold values from 0.099609375 to 1.8984375
- routes: int32 [32768, 4], P(('sp', 'tp')), may hold values from 0 to 63, all different within a row; in each aligned block of 128 rows (0 to 127, 128 to 255, ...) at most 12 rows name the same one
- route_weights: float32 [32768, 4], P(('sp', 'tp')), may hold values from 0.1 to 1
Outputs:
- layer_out: bfloat16 [32768, 2048], P(('sp', 'tp'))
The draws below stay inside these ranges and needn't reach their ends.
Inputs may be any that keep to these rules, and one draw needn't show every extreme that they name: `routes`: each row names 4 different experts. Within the rows of one device (aligned blocks), no expert is named by more than 12 rows, and in some block one expert is named by exactly 12 rows.
All inputs are finite; a program needn't handle non-finite values.
Results may differ from the reference program's by a relative error of at most 0.007.
Values may be sent and summed in bfloat16 or wider, within the bound.
A program may use at most 128 MiB of HBM per device.

```python
import math
import jax
import jax.numpy as jnp
import numpy as np
from jax import lax

D = 2048
CONV_CH = 1024
EXPERT_HIDDEN = 512
SHARED_HIDDEN = 256
CONV_WIDTH = 3
TOPK = 4
TOK_DEV = 512
EXPERTS = 64
CAP = 12
TOKENS = 32768
N_SP = 64
N_TP = 4


def column_scale(key, count):
    ramp = 3.0 ** (jnp.arange(count, dtype=jnp.float32) / count)
    rough = 10.0 ** jax.random.uniform(key, (count,), jnp.float32)
    return ramp * rough / 10.0


def draw_expert_down(key, part):
    first, second = jax.random.split(key)
    base = jnp.clip(jax.random.normal(first, (EXPERTS, EXPERT_HIDDEN, D), jnp.float32), -6.0, 6.0)
    return (base * EXPERT_HIDDEN ** (-0.5) * column_scale(second, D)[None, None, :]).astype(jnp.bfloat16)


def draw_shared_down(key, part):
    first, second = jax.random.split(key)
    base = jnp.clip(jax.random.normal(first, (SHARED_HIDDEN, D), jnp.float32), -6.0, 6.0)
    return (base * SHARED_HIDDEN ** (-0.5) * column_scale(second, D)[None, :]).astype(jnp.bfloat16)


def levels(rng, dims, shards, low, top_value):
    gain, own = 1.0, jax.random.fold_in(rng, 6)
    for dim, blocks in shards:
        steps = jnp.exp(jax.random.uniform(jax.random.fold_in(own, dim), (blocks,), jnp.float32, low / len(shards), top_value / len(shards)))
        gain = gain * jnp.repeat(steps, dims[dim] // blocks).reshape([-1 if axis == dim else 1 for axis in range(len(dims))])
    return gain


def assign_block(stream_key, own, number, rows, number_of, top, most, skew):
    order = jax.random.permutation(stream_key, number_of)
    packed, common = load_shares(number_of, rows * top, most, skew, True), load_shares(number_of, rows * top, most, skew, False)
    places = jnp.arange(number_of)

    def named(tallies, rotation):
        used = int((tallies > 0).sum())
        fixed = max(1, used // 4)
        moved = fixed + (places - fixed + rotation * (used - fixed)) % max(1, number_of - fixed)
        return jnp.zeros((number_of,), jnp.int32).at[order[jnp.where(places < fixed, places, moved)]].set(jnp.asarray(tallies, jnp.int32))

    tallies = jnp.where(number % 4 == 0, named(packed, number // 4), named(common, number - number // 4 - 1))
    mixed = jax.random.permutation(jax.random.fold_in(own, 3), number_of)
    giver, sink = mixed[0:number_of // 2 * 2:2], mixed[1:number_of // 2 * 2:2]
    margin = jnp.minimum(tallies[giver] - 1, most - tallies[sink]) // 2
    margin = jnp.where((giver == order[0]) | (sink == order[0]) | (tallies[sink] == 0), 0, jnp.maximum(margin, 0))
    moved = jax.random.randint(jax.random.fold_in(own, 4), (number_of // 2,), 0, 1 << 20) % (margin + 1)
    tallies = tallies.at[giver].add(-moved).at[sink].add(moved)
    members = jnp.searchsorted(jnp.cumsum(tallies), jnp.arange(rows * top), side="right").astype(jnp.int32)
    table = members.reshape(top, rows).T
    table = table[jax.random.permutation(jax.random.fold_in(own, 1), rows)]
    rotation = jax.random.randint(jax.random.fold_in(own, 2), (rows, 1), 0, top)
    return jnp.take_along_axis(table, (jnp.arange(top)[None, :] + rotation) % top, axis=1)


def load_shares(count, total, bound, lean, full):
    loads = [(1 << 20) // math.isqrt(grade ** lean) + 1 for grade in range(1, count + 1)]
    largest = bound if full else min(bound, max(-(-total // count), total * loads[0] // sum(loads)))
    least = 1 if total - largest >= count - 1 else 0
    holding, rest = [largest] + [least] * (count - 1), total - largest - least * (count - 1)
    while rest > 0:
        free = [i for i in range(1, count) if holding[i] < largest] or [i for i in range(1, count) if holding[i] < bound]
        whole, budget = sum([loads[i] for i in free]), rest
        for i in free:
            addition = min(bound - holding[i], max(1, budget * loads[i] // whole), rest)
            holding[i] = holding[i] + addition
            rest = rest - addition
    return np.array(holding)


def centred(own_key, extent, spread, most, pieces=(), kind=jnp.bfloat16):
    level = levels(own_key, extent, pieces, -0.22, 0.18) if pieces else 1.0
    array = jax.random.normal(own_key, extent, jnp.float32) * spread * level
    return jnp.minimum(jnp.maximum(array, -most), most).astype(kind)


def setup_inputs(seed: int = 0) -> dict:
    arg_keys = jax.random.split(jax.random.key(seed), 18)
    x_in = centred(arg_keys[0], (TOKENS, CONV_CH), 1.0, 6.0, ((0, 64), (1, 4)))
    gate_b = centred(arg_keys[1], (TOKENS, CONV_CH), 1.0, 6.0, ((0, 64), (1, 4)))
    gate_c = centred(arg_keys[2], (TOKENS, CONV_CH), 1.0, 6.0, ((0, 64), (1, 4)))
    conv_taps = centred(arg_keys[3], (CONV_WIDTH, CONV_CH), CONV_WIDTH ** -0.5, 3.5, ((1, 4),))
    out_proj = centred(arg_keys[4], (CONV_CH, D), CONV_CH ** -0.5, 0.1875, ((0, 4),))
    mix_gain = jnp.clip(1.0 + 0.18 * jax.random.normal(arg_keys[5], (D,), jnp.float32), 0.099609375, 1.8984375).astype(jnp.bfloat16)
    resid = centred(arg_keys[6], (TOKENS, D), 1.0, 6.0, ((0, 256),))
    pre_gain = jnp.clip(1.0 + 0.18 * jax.random.normal(arg_keys[7], (D,), jnp.float32), 0.099609375, 1.8984375).astype(jnp.bfloat16)
    expert_gate = centred(arg_keys[8], (EXPERTS, D, EXPERT_HIDDEN), D ** -0.5, 0.125, ((0, 64),))
    expert_up = centred(arg_keys[9], (EXPERTS, D, EXPERT_HIDDEN), D ** -0.5, 0.125, ((0, 64),))
    expert_down = draw_expert_down(jax.random.fold_in(arg_keys[17], 71), 0)
    shared_gate = centred(arg_keys[11], (D, SHARED_HIDDEN), D ** -0.5, 0.125)
    shared_up = centred(arg_keys[12], (D, SHARED_HIDDEN), D ** -0.5, 0.125)
    shared_down = draw_shared_down(jax.random.fold_in(arg_keys[17], 71), 0)
    post_gain = jnp.clip(1.0 + 0.18 * jax.random.normal(arg_keys[14], (D,), jnp.float32), 0.099609375, 1.8984375).astype(jnp.bfloat16)
    routes_keys = jax.random.split(jax.random.fold_in(arg_keys[15], 1), TOKENS // (TOK_DEV // N_TP))
    routes_turns = jax.random.permutation(jax.random.fold_in(arg_keys[15], 3), TOKENS // (TOK_DEV // N_TP))
    routes = jax.vmap(lambda own, number: assign_block(jax.random.fold_in(arg_keys[15], 2), own, number, TOK_DEV // N_TP, EXPERTS, TOPK, CAP, 2))(routes_keys, routes_turns).reshape((TOKENS, TOPK))
    route_weights = jnp.clip(0.1 + 0.9 * jax.random.uniform(arg_keys[16], (TOKENS, TOPK), jnp.float32) ** levels(arg_keys[16], (TOKENS, TOPK), ((0, 256),), -0.2, 0.2), 0.1, 1.0)
    return dict(x_in=x_in, gate_b=gate_b, gate_c=gate_c, conv_taps=conv_taps, out_proj=out_proj, mix_gain=mix_gain, resid=resid, pre_gain=pre_gain, expert_gate=expert_gate, expert_up=expert_up, expert_down=expert_down, shared_gate=shared_gate, shared_up=shared_up, shared_down=shared_down, post_gain=post_gain, routes=routes, route_weights=route_weights)


epsilon = 1e-06

def reference(x_in, gate_b, gate_c, conv_taps, out_proj, mix_gain, resid, pre_gain, expert_gate, expert_up, expert_down, shared_gate, shared_up, shared_down, post_gain, routes, route_weights):
    mixed_in = gate_c.astype(jnp.float32) * x_in.astype(jnp.float32)
    reach = CONV_WIDTH - 1
    padded = jnp.concatenate([jnp.zeros((reach, CONV_CH), jnp.float32), mixed_in], 0)
    taps = conv_taps.astype(jnp.float32)
    convolved = jnp.zeros((TOKENS, CONV_CH), jnp.float32)
    for index in range(CONV_WIDTH):
        convolved = convolved + taps[index][None, :] * padded[index:index + TOKENS]
    conv_out = (gate_b.astype(jnp.float32) * convolved).astype(jnp.bfloat16)
    projected = jnp.dot(conv_out, out_proj, preferred_element_type=jnp.float32)
    row_scale = lax.rsqrt(lax.optimization_barrier(jnp.mean(projected * projected, axis=1, keepdims=True)) + epsilon)
    resid1 = (resid.astype(jnp.float32) + projected * row_scale * mix_gain.astype(jnp.float32)).astype(jnp.bfloat16)
    wide_resid = resid1.astype(jnp.float32)
    normed = (wide_resid * lax.rsqrt(lax.optimization_barrier(jnp.mean(wide_resid * wide_resid, axis=1, keepdims=True)) + epsilon) * pre_gain.astype(jnp.float32)).astype(jnp.bfloat16)
    block_count = N_SP * N_TP
    quarter = TOK_DEV // N_TP
    flat_ids = routes.reshape(-1).astype(jnp.int32)
    onehot = (flat_ids[:, None] == jnp.arange(EXPERTS, dtype=jnp.int32)[None, :]).astype(jnp.int32)
    blocks = onehot.reshape(block_count, quarter * TOPK, EXPERTS)
    before = (jnp.cumsum(blocks, axis=1) - blocks).reshape(-1, EXPERTS)
    position = lax.optimization_barrier(jnp.sum(before * onehot, axis=1))
    source = jnp.arange(TOKENS * TOPK, dtype=jnp.int32) // (quarter * TOPK)
    slot_index = flat_ids * (block_count * CAP) + source * CAP + position
    dispatched = jnp.zeros((EXPERTS * block_count * CAP, D), jnp.bfloat16).at[slot_index].set(jnp.repeat(normed, TOPK, axis=0))

    def run_expert(operands):
        rows_in, w_gate, w_up, w_down = operands
        gate_h = jnp.dot(rows_in, w_gate, preferred_element_type=jnp.float32)
        up_h = jnp.dot(rows_in, w_up, preferred_element_type=jnp.float32)
        hidden = (jax.nn.silu(gate_h) * up_h).astype(jnp.bfloat16)
        return jnp.dot(hidden, w_down, preferred_element_type=jnp.float32).astype(jnp.bfloat16)
    expert_out = lax.map(run_expert, (dispatched.reshape(EXPERTS, block_count * CAP, D), expert_gate, expert_up, expert_down)).reshape(-1, D)
    picked = expert_out[slot_index].reshape(TOKENS, TOPK, D)
    routed = jnp.zeros((TOKENS, D), jnp.float32)
    for index in range(TOPK):
        routed = routed + route_weights[:, index:index + 1] * picked[:, index].astype(jnp.float32)
    shared_g = jnp.dot(normed, shared_gate, preferred_element_type=jnp.float32)
    shared_u = jnp.dot(normed, shared_up, preferred_element_type=jnp.float32)
    shared_hidden = (jax.nn.silu(shared_g) * shared_u).astype(jnp.bfloat16)
    shared_out = jnp.dot(shared_hidden, shared_down, preferred_element_type=jnp.float32)
    branch = routed + shared_out
    factor = lax.rsqrt(lax.optimization_barrier(jnp.mean(branch * branch, axis=1, keepdims=True)) + epsilon)
    return (wide_resid + branch * factor * post_gain.astype(jnp.float32)).astype(jnp.bfloat16)
```

```python
import jax
import jax.numpy as jnp
from jax import lax
from jax.experimental import pallas as pl
from jax.experimental.pallas import tpu as pltpu
from jax.sharding import Mesh
from jax.sharding import PartitionSpec as P

SP = ("sp_0", "sp_1", "sp_2")
SP_TP = ("sp_0", "sp_1", "sp_2", "tp")
MESH = pl.DeviceIdType.MESH

epsilon = 1e-06

Z, X, C, Y = 8, 4, 2, 4
PLANE = X * C
CAP = 12
SIDE = 2
ROWS = SIDE * CAP
SLOTS = PLANE * ROWS
GROUPS = Z // 2
META = 256
TILE = 8
TILES = ROWS // TILE
STRIP = PLANE * TILE
LATE = 2
UNITS = 4


def row_of(ref):
    rows = ref[...].astype(jnp.float32)
    return jnp.concatenate([rows[i : i + 1] for i in range(rows.shape[0])], axis=1)


def fill_tables(meta, routes, route_weights):
    top, tokens = routes.shape
    f32, bf16 = jnp.float32, jnp.bfloat16
    experts = Z * PLANE
    expert = lax.broadcasted_iota(jnp.int32, (experts, tokens), 0)
    named = jnp.zeros((experts, tokens), f32)
    weight = jnp.zeros((experts, tokens), f32)
    for k in range(top):
        hot = expert == routes[k : k + 1]
        named = named + jnp.where(hot, 1.0, 0.0)
        weight = weight + jnp.where(hot, route_weights[k : k + 1], 0.0)
    named = named.T
    weight = weight.T
    row = lax.broadcasted_iota(jnp.int32, (tokens, tokens), 0)
    column = lax.broadcasted_iota(jnp.int32, (tokens, tokens), 1)
    below = jnp.where(row > column, 1.0, 0.0).astype(bf16)
    before = jnp.dot(below, named.astype(bf16), preferred_element_type=f32)
    place = jnp.where(named > 0.0, before, 100.0).astype(bf16)
    high = weight.astype(bf16)
    low = (weight - high.astype(f32)).astype(bf16)
    lane = lax.broadcasted_iota(jnp.int32, (experts, META), 1)
    expert = lax.broadcasted_iota(jnp.int32, (experts, META), 0)

    owner = (lane // TILE) % PLANE
    at = (lane // STRIP) * TILE + lane % TILE
    first = LATE * TILE
    spare = first - CAP
    own_at = jnp.where(at < first, at + TILE, at - first)
    far_at = jnp.where(at < first, at - spare, -1)
    token = lax.broadcasted_iota(jnp.int32, (tokens, META), 0).astype(f32) + 1.0
    z = lax.axis_index("sp_0")
    meta[...] = jnp.zeros_like(meta)
    for by in range(Z):
        side = 1 if by >= GROUPS else 0
        held = (far_at if side else own_at) if by % GROUPS == 0 else at - side * CAP
        within = held[0:1].astype(f32)
        spread = jnp.where(expert - owner == lax.rem(z + by, Z) * PLANE, 1.0, 0.0).astype(bf16)
        put = jnp.dot(place, spread, preferred_element_type=f32) == within
        tags = jnp.where(put, token + side * tokens, 0.0)
        weights = jnp.dot(high, spread, preferred_element_type=f32) + jnp.dot(
            low, spread, preferred_element_type=f32
        )
        meta[by, 0:1] = jnp.sum(tags, axis=0, keepdims=True)
        meta[by, 1:2] = jnp.sum(jnp.where(put, weights, 0.0), axis=0, keepdims=True)


def layer_kernel(
    taps,
    mix_gain,
    pre_gain,
    post_gain,
    routes,
    route_weights,
    x_hbm,
    gb_hbm,
    gc_hbm,
    proj_hbm,
    resid_hbm,
    wg_hbm,
    wu_hbm,
    wd_hbm,
    sg_hbm,
    su_hbm,
    sd_hbm,
    out,
    x_in,
    gb,
    gc,
    edge,
    mixed,
    conv,
    conv_in,
    proj,
    resid,
    normed,
    ag,
    meta,
    tables,
    xs,
    xr,
    fo,
    rr,
    part,
    far,
    rs,
    rv,
    acc,
    wg,
    wu,
    wd,
    sg,
    su,
    sd,
    load_sem,
    local_sem,
    edge_s,
    edge_r,
    conv_s,
    conv_r,
    wy_s,
    wy_r,
    wx_s,
    wx_r,
    wc_s,
    wc_r,
    ag_s,
    ag_r,
    meta_s,
    meta_r,
    x_s,
    x_r,
    e_s,
    e_r,
    b_s,
    b_r,
    l_s,
    l_r,
    h_s,
    h_r,
    rs_s,
    rs_r,
):
    z, x, c, y = (lax.axis_index(a) for a in SP_TP)
    me8 = x * C + c
    sp = z * PLANE + me8
    tokens, width = normed.shape
    half = width // 2

    def z_peer(by):
        return (lax.rem(z + by + Z, Z), x, c, y)

    def y_peer(by):
        return (z, x, c, lax.rem(y + by + Y, Y))

    def plane_peer(j):
        e = lax.rem(me8 + j, PLANE)
        return e, (z, e // C, lax.rem(e, C), y)

    def sp_peer(by):
        to = lax.rem(sp + by + Z * PLANE, Z * PLANE)
        return (to // PLANE, lax.rem(to, PLANE) // C, lax.rem(to, C), y)

    ahead = (z_peer(1), z_peer(-1))
    partner = (z, x, 1 - c, y)
    beside = ((z, lax.rem(x + 1, X), c, y), (z, lax.rem(x + X - 1, X), c, y))

    pairs = (
        (x_hbm, x_in),
        (gc_hbm, gc),
        (proj_hbm, proj.at[0]),
        (gb_hbm, gb),
        (resid_hbm, resid),
        (sg_hbm, sg),
        (su_hbm, su),
        (sd_hbm, sd),
        (wg_hbm, wg),
        (wu_hbm, wu),
        (wd_hbm, wd),
    )
    loads = [
        pltpu.make_async_copy(src, dst, load_sem.at[i]) for i, (src, dst) in enumerate(pairs)
    ]
    for load in loads:
        load.start()

    barrier = pltpu.get_barrier_semaphore()
    greeted = [z_peer(by) for by in range(1, Z)]
    greeted += [plane_peer(j)[1] for j in range(1, PLANE)]
    greeted += [y_peer(by) for by in range(1, Y)]
    greeted += [sp_peer(1), sp_peer(-1)]
    for device in greeted:
        pl.semaphore_signal(barrier, inc=1, device_id=device, device_id_type=MESH)
    pl.semaphore_wait(barrier, len(greeted))

    def remote(src, dst, send, recv, device):
        return pltpu.make_async_remote_copy(
            src_ref=src,
            dst_ref=dst,
            send_sem=send,
            recv_sem=recv,
            device_id=device,
            device_id_type=MESH,
        )

    started = []

    def begin(copy):
        copy.start()
        started.append(copy)
        return copy

    count, channels = x_in.shape
    loads[0].wait()
    loads[1].wait()
    edges = [
        begin(
            remote(
                ref.at[pl.ds(count - 8, 8)], edge.at[i], edge_s.at[i], edge_r.at[i], sp_peer(1)
            )
        )
        for i, ref in enumerate((x_in, gc))
    ]

    unit = proj.shape[1] // 8
    parity = lax.rem(x, 2)

    def unit_rows(core, par, sub):
        return pl.ds(pl.multiple_of((core * 4 + par * 2 + sub) * unit, unit), unit)

    def y_unit(source, by, sub):
        way = 1 if (by == 1 or (by == 2 and sub == 0)) else -1
        rows_at = unit_rows(c, parity, sub)
        return remote(
            proj.at[source, rows_at],
            proj.at[by, rows_at],
            wy_s.at[by, sub],
            wy_r.at[by, sub],
            y_peer(way),
        )

    loads[2].wait()
    units = {}
    for by, sub in ((1, 0), (3, 1), (1, 1), (3, 0)):
        units[by, sub] = begin(y_unit(0, by, sub))

    loads[3].wait()
    mixed[8 : 8 + count] = gc[...].astype(jnp.float32) * x_in[...].astype(jnp.float32)
    for copy in edges:
        copy.wait_recv()
    before = edge[1].astype(jnp.float32) * edge[0].astype(jnp.float32)
    mixed[0:8] = jnp.where(sp > 0, before, 0.0)
    reach = taps.shape[0] - 1
    tap = taps[...].astype(jnp.float32)
    convolved = tap[0:1] * mixed[8 - reach : 8 - reach + count]
    for index in range(1, reach + 1):
        at = 8 - reach + index
        convolved = convolved + tap[index : index + 1] * mixed[at : at + count]
    conv[...] = (gb[...].astype(jnp.float32) * convolved).astype(jnp.bfloat16)

    def token_rows(owner):
        return pl.ds(pl.multiple_of(owner * tokens, tokens), tokens)

    fill_tables(meta, routes, route_weights)

    def table_copy(by):
        group = by if by < GROUPS else (Z - by) % GROUPS
        slot = group * SIDE + (1 if by >= GROUPS else 0)
        return remote(meta.at[by], tables.at[slot], meta_s.at[by], meta_r.at[slot], z_peer(by))

    table_copies = [table_copy(by) for by in range(1, Z)]
    for copy in table_copies:
        copy.start()
    own_table = pltpu.make_async_copy(meta.at[0], tables.at[0], local_sem.at[1])
    own_table.start()

    def x_unit(by, sub):
        rows_at = unit_rows(c, parity, sub)
        return remote(
            proj.at[by, rows_at],
            proj.at[by, rows_at],
            wx_s.at[by, sub],
            wx_r.at[by, sub],
            beside[sub],
        )

    def core_unit(by, kind, sub):
        rows_at = unit_rows(c, parity if kind == 0 else 1 - parity, sub)
        return remote(
            proj.at[by, rows_at],
            proj.at[by, rows_at],
            wc_s.at[by, kind, sub],
            wc_r.at[by, kind, sub],
            partner,
        )

    def conv_copy(by):
        return remote(
            conv.at[token_rows(lax.rem(y + by, Y))],
            conv_in.at[by],
            conv_s.at[by],
            conv_r.at[by],
            y_peer(by),
        )

    conv_copies = []
    sides, swaps = {}, []
    waiting = []

    def side_arrived(key):
        sides[key].wait_recv()
        swaps.append(begin(core_unit(key[0], 1, key[1])))

    for by, sub in ((1, 0), (3, 1), (1, 1), (3, 0), (2, 0), (2, 1)):
        units[by, sub].wait_recv()
        if (by, sub) in ((1, 0), (3, 1)):
            units[2, sub] = begin(y_unit(by, 2, sub))
            if sub == 1:
                for to in range(1, Y):
                    conv_copies.append(begin(conv_copy(to)))
        sides[by, sub] = begin(x_unit(by, sub))
        swaps.append(begin(core_unit(by, 0, sub)))
        waiting.append((by, sub))
        if len(waiting) > 2:
            side_arrived(waiting.pop(0))
    for key in waiting:
        side_arrived(key)
    part[0:tokens] = jnp.dot(
        conv[token_rows(y)], proj[0], preferred_element_type=jnp.float32
    )
    for copy in conv_copies + swaps:
        copy.wait_recv()
    projected = part[0:tokens]
    for by in range(1, Y):
        projected = projected + jnp.dot(
            conv_in[by], proj[by], preferred_element_type=jnp.float32
        )
    loads[4].wait()
    row_scale = lax.rsqrt(jnp.mean(projected * projected, axis=1, keepdims=True) + epsilon)
    resid1 = (resid[...].astype(jnp.float32) + projected * row_scale * row_of(mix_gain)).astype(
        jnp.bfloat16
    )
    resid[...] = resid1
    wide_resid = resid1.astype(jnp.float32)
    normed[...] = (
        wide_resid
        * lax.rsqrt(jnp.mean(wide_resid * wide_resid, axis=1, keepdims=True) + epsilon)
        * row_of(pre_gain)
    ).astype(jnp.bfloat16)

    def gather_copy(src, group, side, chunk, way, step):
        return remote(
            src,
            ag.at[group, pl.ds(side * tokens, tokens), pl.ds(chunk * half, half)],
            ag_s.at[way, step, chunk],
            ag_r.at[way, step, chunk],
            ahead[way],
        )

    arriving = {}
    for chunk in range(2):
        for way in range(2):
            src = normed.at[pl.ds(0, tokens), pl.ds(chunk * half, half)]
            arriving[way, chunk] = begin(gather_copy(src, 1, way, chunk, way, 0))
    own_rows = pltpu.make_async_copy(normed, ag.at[0, pl.ds(0, tokens)], local_sem.at[0])
    own_rows.start()

    def slots_copies(src, dst, group, tiles, cols, send, recv):
        def view(ref, e):
            strip = pl.ds(pl.multiple_of(e * TILE, TILE), TILE)
            return ref.at[group, pl.ds(tiles[0], tiles[1] - tiles[0]), strip, pl.ds(*cols)]

        copies = []
        for j in range(1, PLANE):
            e, device = plane_peer(j)
            copies.append(remote(view(src, e), view(dst, me8), send(j), recv(j), device))
        copies.append(pltpu.make_async_copy(view(src, me8), view(dst, me8), send(0)))
        for copy in copies:
            copy.start()
        return copies

    whole = (0, width)
    halves = ((0, half), (half, half))

    def finish(copies):
        for copy in copies:
            copy.wait()

    f32, bf16 = jnp.float32, jnp.bfloat16
    late_rows = LATE * STRIP

    own_table.wait()
    token = lax.broadcasted_iota(jnp.int32, (tokens, SLOTS - late_rows), 0).astype(f32)
    chosen = jnp.where(token + 1.0 == tables[0, 0:1, late_rows:SLOTS], 1.0, 0.0).astype(bf16)
    xs[0, LATE] = lax.dot_general(
        chosen, normed[...], (((0,), (0,)), ((), ())), preferred_element_type=f32
    ).astype(bf16)
    early = slots_copies(
        xs, xr, 0, (LATE, TILES), whole, lambda j: e_s.at[j], lambda j: e_r.at[j]
    )

    for load in loads[5:8]:
        load.wait()
    rows = normed[...]
    shared_g = jnp.dot(rows, sg[...], preferred_element_type=f32)
    shared_u = jnp.dot(rows, su[...], preferred_element_type=f32)
    shared_h = (shared_g * jax.nn.sigmoid(shared_g) * shared_u).astype(bf16)
    acc[...] = jnp.dot(shared_h, sd[...], preferred_element_type=f32)
    for load in loads[8:]:
        load.wait()
    own_rows.wait()
    finish(table_copies)

    def table(group, row, tiles):
        both = tables[2 * group] + tables[2 * group + 1]
        if tiles[0]:
            both = pltpu.roll(both, META - tiles[0] * STRIP, 1)
        return both[row : row + 1, 0 : (tiles[1] - tiles[0]) * STRIP]

    def hits(group, rows, tiles):
        first, last = rows
        shape = (last - first, (tiles[1] - tiles[0]) * STRIP)
        row = lax.broadcasted_iota(jnp.int32, shape, 0).astype(f32)
        return row + (first + 1.0) == table(group, 0, tiles)

    def dispatch(group, chunk, tiles):
        picks = jnp.where(hits(group, (0, 2 * tokens), tiles), 1.0, 0.0).astype(bf16)
        cols = slice(chunk * half, (chunk + 1) * half)
        xs[group, tiles[0] : tiles[1], :, cols] = (
            lax.dot_general(
                picks,
                ag[group, :, cols],
                (((0,), (0,)), ((), ())),
                preferred_element_type=f32,
            )
            .astype(bf16)
            .reshape(tiles[1] - tiles[0], STRIP, half)
        )
        return slots_copies(
            xs,
            xr,
            group,
            tiles,
            halves[chunk],
            lambda j: x_s.at[group, chunk, j],
            lambda j: x_r.at[group, chunk, j],
        )

    def experts(group, tiles):
        count = tiles[1] - tiles[0]
        rows_in = xr[group, tiles[0] : tiles[1]].reshape(count * STRIP, width)
        gate_h = jnp.dot(rows_in, wg[...], preferred_element_type=f32)
        up_h = jnp.dot(rows_in, wu[...], preferred_element_type=f32)
        hidden = (gate_h * jax.nn.sigmoid(gate_h) * up_h).astype(bf16)
        fo[group, tiles[0] : tiles[1]] = (
            jnp.dot(hidden, wd[...], preferred_element_type=f32)
            .astype(bf16)
            .reshape(count, STRIP, width)
        )

    def give(group, tiles):
        return slots_copies(
            fo, rr, group, tiles, whole, lambda j: b_s.at[group, j], lambda j: b_r.at[group, j]
        )

    def give_part(tiles, chunk, part_no):
        return slots_copies(
            fo,
            rr,
            GROUPS - 1,
            tiles,
            halves[chunk],
            lambda j: h_s.at[part_no, chunk, j],
            lambda j: h_r.at[part_no, chunk, j],
        )

    def combine(group, rows, tiles, cols):
        weights = jnp.where(hits(group, rows, tiles), table(group, 1, tiles), 0.0)
        high = weights.astype(bf16)
        low = (weights - high.astype(f32)).astype(bf16)
        at, size = cols
        back = rr[group, tiles[0] : tiles[1], :, at : at + size]
        back = back.reshape((tiles[1] - tiles[0]) * STRIP, size)
        return jnp.dot(high, back, preferred_element_type=f32) + jnp.dot(
            low, back, preferred_element_type=f32
        )

    every, later, side_tiles = (0, TILES), (0, LATE), ((0, 2), (1, 3))

    dealt = {}
    for step in range(1, GROUPS):
        passed = {}
        dealt[step] = []
        farthest = step == GROUPS - 1
        for chunk in range(2):
            for way in range(2):
                arriving[way, chunk].wait_recv()
                if farthest and chunk != way:
                    continue
                src = ag.at[step, pl.ds(way * tokens, tokens), pl.ds(chunk * half, half)]
                group, side = (0, 1) if farthest else (step + 1, way)
                passed[way, chunk] = begin(gather_copy(src, group, side, chunk, way, step))
            dealt[step] += dispatch(step, chunk, every)
            if chunk == 0 and step > 1:
                finish(dealt[step - 1])
                experts(step - 1, every)
        arriving = passed
    dealt[0] = []
    for chunk in range(2):
        arriving[chunk, chunk].wait_recv()
        dealt[0] += dispatch(0, chunk, later)
    last = GROUPS - 1
    finish(dealt[last])
    experts(last, every)
    given = {(last, 0): give_part(side_tiles[0], 1, 0) + give_part(side_tiles[1], 0, 0)}
    finish(dealt[0])
    experts(0, later)
    given[0] = give(0, later)
    given[last, 1] = give_part((2, 3), 1, 1) + give_part((0, 1), 0, 1)
    for group in range(last - 1, 0, -1):
        given[group] = give(group, every)
    finish(early)
    experts(0, (LATE, TILES))
    given_early = slots_copies(
        fo, rr, 0, (LATE, TILES), whole, lambda j: l_s.at[j], lambda j: l_r.at[j]
    )

    unit_cols = width // UNITS

    def send_on(side, hop, no, total):
        cols = pl.ds(no * unit_cols, unit_cols)
        rs[side, hop, :, no * unit_cols : (no + 1) * unit_cols] = total.astype(bf16)
        return begin(
            remote(
                rs.at[side, hop, pl.ds(0, tokens), cols],
                rv.at[side, hop, pl.ds(0, tokens), cols],
                rs_s.at[side, hop, no],
                rs_r.at[side, hop, no],
                ahead[1 - side],
            )
        )

    def own_term(side, no):
        return part[
            side * tokens : (side + 1) * tokens, no * unit_cols : (no + 1) * unit_cols
        ]

    def came(side, hop, no):
        return rv[side, hop, :, no * unit_cols : (no + 1) * unit_cols].astype(f32)

    def units_of(chunk):
        return range(chunk * UNITS // 2, (chunk + 1) * UNITS // 2)

    def add_on(coming, passed, hop, flip):
        for one, two in zip(units_of(flip), units_of(1 - flip)):
            for side, no in ((0, one), (1, two)):
                total = own_term(side, no)
                if (side, no) in coming:
                    coming[side, no].wait_recv()
                    total = total + came(side, hop - 1, no)
                passed[side, no] = send_on(side, hop, no, total)

    def side_rows(side):
        return (side * tokens, (side + 1) * tokens)

    coming, passed = {}, {}
    finish(given[last, 0])
    for side in range(2):
        at = (1 - side) * half
        part[side * tokens : (side + 1) * tokens, at : at + half] = combine(
            last, side_rows(side), side_tiles[side], (at, half)
        )
    add_on(coming, passed, 1, 1)
    finish(given[0])
    far[...] = combine(0, side_rows(1), later, whole)
    for one, two in zip(units_of(0), units_of(1)):
        for side, no in ((0, one), (1, two)):
            value = far[:, no * unit_cols : (no + 1) * unit_cols]
            coming[side, no] = send_on(side, 0, no, value)
    finish(given[last, 1])
    for side in range(2):
        at = side * half
        part[side * tokens : (side + 1) * tokens, at : at + half] = combine(
            last, side_rows(side), side_tiles[side], (at, half)
        )
    add_on(coming, passed, 1, 0)
    for hop in range(2, GROUPS):
        coming, passed = passed, {}
        group = GROUPS - hop
        finish(given[group])
        part[...] = combine(group, (0, 2 * tokens), every, whole)
        add_on(coming, passed, hop, 1)
        add_on(coming, passed, hop, 0)
    finish(given_early)
    acc[...] += combine(0, side_rows(0), every, whole)
    for flip in (1, 0):
        for one, two in zip(units_of(flip), units_of(1 - flip)):
            for side, no in ((0, one), (1, two)):
                passed[side, no].wait_recv()
                acc[:, no * unit_cols : (no + 1) * unit_cols] += came(side, last, no)

    branch = acc[...]
    factor = lax.rsqrt(jnp.mean(branch * branch, axis=1, keepdims=True) + epsilon)
    out[...] = (resid[...].astype(jnp.float32) + branch * factor * row_of(post_gain)).astype(
        jnp.bfloat16
    )
    for copy in started:
        copy.wait_send()


def body(
    x_in,
    gate_b,
    gate_c,
    conv_taps,
    out_proj,
    mix_gain,
    resid,
    pre_gain,
    expert_gate,
    expert_up,
    expert_down,
    shared_gate,
    shared_up,
    shared_down,
    post_gain,
    routes,
    route_weights,
):
    tokens, width = resid.shape
    rows, channels = x_in.shape
    hidden = expert_gate.shape[2]
    shared = shared_gate.shape[1]
    bf16, f32 = jnp.bfloat16, jnp.float32
    vmem = pl.BlockSpec(memory_space=pltpu.VMEM)
    hbm = pl.BlockSpec(memory_space=pl.ANY)
    dma = pltpu.SemaphoreType.DMA
    return pl.pallas_call(
        layer_kernel,
        out_shape=pltpu.VMEM((tokens, width), bf16),
        in_specs=[vmem] * 6 + [hbm] * 11,
        out_specs=vmem,
        scratch_shapes=[
            pltpu.VMEM((rows, channels), bf16),
            pltpu.VMEM((rows, channels), bf16),
            pltpu.VMEM((rows, channels), bf16),
            pltpu.VMEM((2, 8, channels), bf16),
            pltpu.VMEM((rows + 8, channels), f32),
            pltpu.VMEM((rows, channels), bf16),
            pltpu.VMEM((Y, tokens, channels), bf16),
            pltpu.VMEM((Y, channels, width), bf16),
            pltpu.VMEM((tokens, width), bf16),
            pltpu.VMEM((tokens, width), bf16),
            pltpu.VMEM((GROUPS, 2 * tokens, width), bf16),
            pltpu.VMEM((Z, 8, META), f32),
            pltpu.VMEM((Z, 8, META), f32),
            pltpu.VMEM((GROUPS, TILES, STRIP, width), bf16),
            pltpu.VMEM((GROUPS, TILES, STRIP, width), bf16),
            pltpu.VMEM((GROUPS, TILES, STRIP, width), bf16),
            pltpu.VMEM((GROUPS, TILES, STRIP, width), bf16),
            pltpu.VMEM((2 * tokens, width), f32),
            pltpu.VMEM((tokens, width), f32),
            pltpu.VMEM((2, GROUPS, tokens, width), bf16),
            pltpu.VMEM((2, GROUPS, tokens, width), bf16),
            pltpu.VMEM((tokens, width), f32),
            pltpu.VMEM((width, hidden), bf16),
            pltpu.VMEM((width, hidden), bf16),
            pltpu.VMEM((hidden, width), bf16),
            pltpu.VMEM((width, shared), bf16),
            pltpu.VMEM((width, shared), bf16),
            pltpu.VMEM((shared, width), bf16),
            dma((11,)),
            dma((2,)),
            dma((2,)),
            dma((2,)),
            dma((Y,)),
            dma((Y,)),
            dma((Y, 2)),
            dma((Y, 2)),
            dma((Y, 2)),
            dma((Y, 2)),
            dma((Y, 2, 2)),
            dma((Y, 2, 2)),
            dma((2, GROUPS, 2)),
            dma((2, GROUPS, 2)),
            dma((Z,)),
            dma((Z,)),
            dma((GROUPS, 2, PLANE)),
            dma((GROUPS, 2, PLANE)),
            dma((PLANE,)),
            dma((PLANE,)),
            dma((GROUPS, PLANE)),
            dma((GROUPS, PLANE)),
            dma((PLANE,)),
            dma((PLANE,)),
            dma((2, 2, PLANE)),
            dma((2, 2, PLANE)),
            dma((2, GROUPS, UNITS)),
            dma((2, GROUPS, UNITS)),
        ],
        compiler_params=pltpu.CompilerParams(
            collective_id=0, has_side_effects=True, vmem_limit_bytes=63 * 1024 * 1024
        ),
    )(
        conv_taps,
        mix_gain.reshape(-1, 128),
        pre_gain.reshape(-1, 128),
        post_gain.reshape(-1, 128),
        routes.T,
        route_weights.T,
        x_in,
        gate_b,
        gate_c,
        out_proj,
        resid,
        expert_gate[0],
        expert_up[0],
        expert_down[0],
        shared_gate,
        shared_up,
        shared_down,
    )


def solution(mesh):
    finer = Mesh(mesh.devices.reshape(Z, X, C, mesh.shape["tp"]), SP_TP)
    placed = (
        P(SP, "tp"),
        P(SP, "tp"),
        P(SP, "tp"),
        P(None, "tp"),
        P("tp", None),
        P(),
        P(SP_TP, None),
        P(),
        P(SP, None, None),
        P(SP, None, None),
        P(SP, None, None),
        P(),
        P(),
        P(),
        P(),
        P(SP_TP, None),
        P(SP_TP, None),
    )
    return jax.shard_map(
        body, mesh=finer, in_specs=placed, out_specs=P(SP_TP, None), check_vma=False
    )
```

```python
import jax
import jax.numpy as jnp
from jax import lax
from jax.experimental import pallas as pl
from jax.experimental.pallas import tpu as pltpu
from jax.sharding import Mesh
from jax.sharding import PartitionSpec as P

SP = ("sp_0", "sp_1", "sp_2")
SP_TP = ("sp_0", "sp_1", "sp_2", "tp")
MESH = pl.DeviceIdType.MESH

epsilon = 1e-06

Z, X, C, Y = 8, 4, 2, 4
PLANE = X * C
CAP = 12
SIDE = 2
ROWS = SIDE * CAP
SLOTS = PLANE * ROWS
GROUPS = Z // 2
META = 256
TILE = 8
TILES = ROWS // TILE
STRIP = PLANE * TILE
LATE = 2
PARTS = 4
HOPS = Z - 1
SUBS = 4


def row_of(ref):
    rows = ref[...].astype(jnp.float32)
    return jnp.concatenate([rows[i : i + 1] for i in range(rows.shape[0])], axis=1)


def fill_tables(meta, routes, route_weights):
    top, tokens = routes.shape
    f32, bf16 = jnp.float32, jnp.bfloat16
    experts = Z * PLANE
    expert = lax.broadcasted_iota(jnp.int32, (experts, tokens), 0)
    named = jnp.zeros((experts, tokens), f32)
    weight = jnp.zeros((experts, tokens), f32)
    for k in range(top):
        hot = expert == routes[k : k + 1]
        named = named + jnp.where(hot, 1.0, 0.0)
        weight = weight + jnp.where(hot, route_weights[k : k + 1], 0.0)
    named = named.T
    weight = weight.T
    row = lax.broadcasted_iota(jnp.int32, (tokens, tokens), 0)
    column = lax.broadcasted_iota(jnp.int32, (tokens, tokens), 1)
    below = jnp.where(row > column, 1.0, 0.0).astype(bf16)
    before = jnp.dot(below, named.astype(bf16), preferred_element_type=f32)
    place = jnp.where(named > 0.0, before, 100.0).astype(bf16)
    high = weight.astype(bf16)
    low = (weight - high.astype(f32)).astype(bf16)
    lane = lax.broadcasted_iota(jnp.int32, (experts, META), 1)
    expert = lax.broadcasted_iota(jnp.int32, (experts, META), 0)

    owner = (lane // TILE) % PLANE
    at = (lane // STRIP) * TILE + lane % TILE
    first = LATE * TILE
    spare = first - CAP
    own_at = jnp.where(at < first, at + TILE, at - first)
    far_at = jnp.where(at < first, at - spare, -1)
    token = lax.broadcasted_iota(jnp.int32, (tokens, META), 0).astype(f32) + 1.0
    z = lax.axis_index("sp_0")
    meta[...] = jnp.zeros_like(meta)
    for by in range(Z):
        side = 1 if by >= GROUPS else 0
        held = (far_at if side else own_at) if by % GROUPS == 0 else at - side * CAP
        within = held[0:1].astype(f32)
        spread = jnp.where(expert - owner == lax.rem(z + by, Z) * PLANE, 1.0, 0.0).astype(bf16)
        put = jnp.dot(place, spread, preferred_element_type=f32) == within
        tags = jnp.where(put, token + side * tokens, 0.0)
        weights = jnp.dot(high, spread, preferred_element_type=f32) + jnp.dot(
            low, spread, preferred_element_type=f32
        )
        meta[by, 0:1] = jnp.sum(tags, axis=0, keepdims=True)
        meta[by, 1:2] = jnp.sum(jnp.where(put, weights, 0.0), axis=0, keepdims=True)


def layer_kernel(
    taps,
    mix_gain,
    pre_gain,
    post_gain,
    routes,
    route_weights,
    x_hbm,
    gb_hbm,
    gc_hbm,
    proj_hbm,
    resid_hbm,
    wg_hbm,
    wu_hbm,
    wd_hbm,
    sg_hbm,
    su_hbm,
    sd_hbm,
    out,
    x_in,
    gb,
    gc,
    edge,
    mixed,
    conv,
    conv_in,
    proj,
    resid,
    normed,
    ag,
    meta,
    tables,
    xs,
    xr,
    fo,
    rr,
    part,
    rs,
    rv,
    acc,
    wg,
    wu,
    wd,
    sg,
    su,
    sd,
    load_sem,
    local_sem,
    edge_s,
    edge_r,
    conv_s,
    conv_r,
    wy_s,
    wy_r,
    wx_s,
    wx_r,
    wc_s,
    wc_r,
    ag_s,
    ag_r,
    meta_s,
    meta_r,
    x_s,
    x_r,
    e_s,
    e_r,
    b_s,
    b_r,
    l_s,
    l_r,
    h_s,
    h_r,
    rs_s,
    rs_r,
):
    z, x, c, y = (lax.axis_index(a) for a in SP_TP)
    me8 = x * C + c
    sp = z * PLANE + me8
    tokens, width = normed.shape
    half = width // 2
    share = width // PARTS

    def z_peer(by):
        return (lax.rem(z + by + Z, Z), x, c, y)

    def y_peer(by):
        return (z, x, c, lax.rem(y + by + Y, Y))

    def plane_peer(j):
        e = lax.rem(me8 + j, PLANE)
        return e, (z, e // C, lax.rem(e, C), y)

    def sp_peer(by):
        to = lax.rem(sp + by + Z * PLANE, Z * PLANE)
        return (to // PLANE, lax.rem(to, PLANE) // C, lax.rem(to, C), y)

    ahead = (z_peer(1), z_peer(-1))
    partner = (z, x, 1 - c, y)
    beside = (
        (z, lax.rem(x + 1, X), c, y),
        (z, lax.rem(x + X - 1, X), c, y),
        z_peer(1),
        z_peer(-1),
    )

    pairs = (
        (x_hbm, x_in),
        (gc_hbm, gc),
        (proj_hbm, proj.at[0]),
        (gb_hbm, gb),
        (resid_hbm, resid),
        (sg_hbm, sg),
        (su_hbm, su),
        (sd_hbm, sd),
        (wg_hbm, wg),
        (wu_hbm, wu),
        (wd_hbm, wd),
    )
    loads = [
        pltpu.make_async_copy(src, dst, load_sem.at[i]) for i, (src, dst) in enumerate(pairs)
    ]
    for load in loads:
        load.start()

    barrier = pltpu.get_barrier_semaphore()
    greeted = [z_peer(by) for by in range(1, Z)]
    greeted += [plane_peer(j)[1] for j in range(1, PLANE)]
    greeted += [y_peer(by) for by in range(1, Y)]
    greeted += [sp_peer(1), sp_peer(-1)]
    for device in greeted:
        pl.semaphore_signal(barrier, inc=1, device_id=device, device_id_type=MESH)
    fill_tables(meta, routes, route_weights)
    pl.semaphore_wait(barrier, len(greeted))

    def remote(src, dst, send, recv, device):
        return pltpu.make_async_remote_copy(
            src_ref=src,
            dst_ref=dst,
            send_sem=send,
            recv_sem=recv,
            device_id=device,
            device_id_type=MESH,
        )

    started = []

    def begin(copy):
        copy.start()
        started.append(copy)
        return copy

    count, channels = x_in.shape
    loads[0].wait()
    loads[1].wait()
    edges = [
        begin(
            remote(
                ref.at[pl.ds(count - 8, 8)], edge.at[i], edge_s.at[i], edge_r.at[i], sp_peer(1)
            )
        )
        for i, ref in enumerate((x_in, gc))
    ]

    unit = proj.shape[1] // (2 * C * SUBS)
    parity = lax.rem(x + z, 2)

    def unit_rows(core, par, sub):
        return pl.ds(pl.multiple_of(((core * 2 + par) * SUBS + sub) * unit, unit), unit)

    def y_unit(source, by, sub):
        way = 1 if (by == 1 or (by == 2 and sub < SUBS // 2)) else -1
        rows_at = unit_rows(c, parity, sub)
        return remote(
            proj.at[source, rows_at],
            proj.at[by, rows_at],
            wy_s.at[by, sub],
            wy_r.at[by, sub],
            y_peer(way),
        )

    loads[2].wait()
    units = {}
    near = [(by, (sub + (0 if by == 1 else 2)) % SUBS) for sub in range(SUBS) for by in (1, 3)]
    for by, sub in near:
        units[by, sub] = begin(y_unit(0, by, sub))

    loads[3].wait()
    mixed[8 : 8 + count] = gc[...].astype(jnp.float32) * x_in[...].astype(jnp.float32)
    reach = taps.shape[0] - 1
    tap = taps[...].astype(jnp.float32)
    mixed[0:8] = jnp.zeros((8, channels), jnp.float32)

    def convolve(first, last):
        total = None
        for index in range(reach + 1):
            at = 8 - reach + index
            term = tap[index : index + 1] * mixed[at + first : at + last]
            total = term if total is None else total + term
        conv[first:last] = (gb[first:last].astype(jnp.float32) * total).astype(jnp.bfloat16)

    convolve(0, count)

    def token_rows(owner):
        return pl.ds(pl.multiple_of(owner * tokens, tokens), tokens)

    def table_copy(by):
        group = by if by < GROUPS else (Z - by) % GROUPS
        slot = group * SIDE + (1 if by >= GROUPS else 0)
        return remote(meta.at[by], tables.at[slot], meta_s.at[by], meta_r.at[slot], z_peer(by))

    table_copies = [table_copy(by) for by in range(1, Z)]
    for copy in table_copies:
        copy.start()
    own_table = pltpu.make_async_copy(meta.at[0], tables.at[0], local_sem.at[1])
    own_table.start()

    def x_unit(by, sub):
        rows_at = unit_rows(c, parity, sub)
        return remote(
            proj.at[by, rows_at],
            proj.at[by, rows_at],
            wx_s.at[by, sub],
            wx_r.at[by, sub],
            beside[sub],
        )

    def core_unit(by, kind, sub):
        rows_at = unit_rows(c, parity if kind == 0 else 1 - parity, sub)
        return remote(
            proj.at[by, rows_at],
            proj.at[by, rows_at],
            wc_s.at[by, kind, sub],
            wc_r.at[by, kind, sub],
            partner,
        )

    def conv_copy(by):
        return remote(
            conv.at[token_rows(lax.rem(y + by, Y))],
            conv_in.at[by],
            conv_s.at[by],
            conv_r.at[by],
            y_peer(by),
        )

    conv_copies = []
    sides, swaps = {}, {}
    waiting = []

    def side_arrived(by, sub):
        sides[by, sub].wait_recv()
        swaps[by, 1, sub] = begin(core_unit(by, 1, sub))

    relayed = {(1, 0), (1, 1), (3, 2), (3, 3)}
    for by, sub in near + [(2, 0), (2, 2), (2, 1), (2, 3)]:
        units[by, sub].wait_recv()
        if (by, sub) in relayed:
            units[2, sub] = begin(y_unit(by, 2, sub))
        sides[by, sub] = begin(x_unit(by, sub))
        swaps[by, 0, sub] = begin(core_unit(by, 0, sub))
        waiting.append((by, sub))
        if (by, sub) == (3, 3):
            for copy in edges:
                copy.wait_recv()
            before = edge[1].astype(jnp.float32) * edge[0].astype(jnp.float32)
            mixed[0:8] = jnp.where(sp > 0, before, 0.0)
            convolve(0, 8)
            for to in range(1, Y):
                conv_copies.append(begin(conv_copy(to)))
        if len(waiting) > 4:
            side_arrived(*waiting.pop(0))
    part[0:tokens] = jnp.dot(conv[token_rows(y)], proj[0], preferred_element_type=jnp.float32)
    for by, sub in waiting:
        side_arrived(by, sub)
    for by in (1, 3, 2):
        conv_copies[by - 1].wait_recv()
        for kind in range(2):
            for sub in range(SUBS):
                swaps[by, kind, sub].wait_recv()
        part[0:tokens] += jnp.dot(conv_in[by], proj[by], preferred_element_type=jnp.float32)
    projected = part[0:tokens]
    loads[4].wait()
    row_scale = lax.rsqrt(jnp.mean(projected * projected, axis=1, keepdims=True) + epsilon)
    resid1 = (resid[...].astype(jnp.float32) + projected * row_scale * row_of(mix_gain)).astype(
        jnp.bfloat16
    )
    resid[...] = resid1
    wide_resid = resid1.astype(jnp.float32)
    normed[...] = (
        wide_resid
        * lax.rsqrt(jnp.mean(wide_resid * wide_resid, axis=1, keepdims=True) + epsilon)
        * row_of(pre_gain)
    ).astype(jnp.bfloat16)

    def gather_copy(src, group, side, chunk, way, step):
        return remote(
            src,
            ag.at[group, pl.ds(side * tokens, tokens), pl.ds(chunk * share, share)],
            ag_s.at[way, step, chunk],
            ag_r.at[way, step, chunk],
            ahead[way],
        )

    arriving = {}
    for chunk in range(PARTS):
        for way in range(2):
            src = normed.at[pl.ds(0, tokens), pl.ds(chunk * share, share)]
            arriving[way, chunk] = begin(gather_copy(src, 1, way, chunk, way, 0))
    own_rows = pltpu.make_async_copy(normed, ag.at[0, pl.ds(0, tokens)], local_sem.at[0])
    own_rows.start()

    def slots_copies(src, dst, group, tiles, cols, send, recv):
        def view(ref, e):
            strip = pl.ds(pl.multiple_of(e * TILE, TILE), TILE)
            return ref.at[group, pl.ds(tiles[0], tiles[1] - tiles[0]), strip, pl.ds(*cols)]

        copies = []
        for j in range(1, PLANE):
            e, device = plane_peer(j)
            copies.append(remote(view(src, e), view(dst, me8), send(j), recv(j), device))
        copies.append(pltpu.make_async_copy(view(src, me8), view(dst, me8), send(0)))
        for copy in copies:
            copy.start()
        return copies

    whole = (0, width)
    halves = ((0, half), (half, half))

    def finish(copies):
        for copy in copies:
            copy.wait()

    f32, bf16 = jnp.float32, jnp.bfloat16
    late_rows = LATE * STRIP

    own_table.wait()
    token = lax.broadcasted_iota(jnp.int32, (tokens, SLOTS - late_rows), 0).astype(f32)
    chosen = jnp.where(token + 1.0 == tables[0, 0:1, late_rows:SLOTS], 1.0, 0.0).astype(bf16)
    xs[0, LATE] = lax.dot_general(
        chosen, normed[...], (((0,), (0,)), ((), ())), preferred_element_type=f32
    ).astype(bf16)
    early = slots_copies(
        xs, xr, 0, (LATE, TILES), whole, lambda j: e_s.at[j], lambda j: e_r.at[j]
    )

    for load in loads[5:8]:
        load.wait()
    rows = normed[...]
    shared_g = jnp.dot(rows, sg[...], preferred_element_type=f32)
    shared_u = jnp.dot(rows, su[...], preferred_element_type=f32)
    shared_h = (shared_g * jax.nn.sigmoid(shared_g) * shared_u).astype(bf16)
    acc[...] = jnp.dot(shared_h, sd[...], preferred_element_type=f32)
    for load in loads[8:]:
        load.wait()
    own_rows.wait()
    finish(table_copies)

    def table(group, row, tiles):
        both = tables[2 * group] + tables[2 * group + 1]
        if tiles[0]:
            both = pltpu.roll(both, META - tiles[0] * STRIP, 1)
        return both[row : row + 1, 0 : (tiles[1] - tiles[0]) * STRIP]

    def hits(group, rows, tiles):
        first, last = rows
        shape = (last - first, (tiles[1] - tiles[0]) * STRIP)
        row = lax.broadcasted_iota(jnp.int32, shape, 0).astype(f32)
        return row + (first + 1.0) == table(group, 0, tiles)

    def dispatch(group, chunk, tiles):
        picks = jnp.where(hits(group, (0, 2 * tokens), tiles), 1.0, 0.0).astype(bf16)
        cols = slice(chunk * share, (chunk + 1) * share)
        xs[group, tiles[0] : tiles[1], :, cols] = (
            lax.dot_general(
                picks,
                ag[group, :, cols],
                (((0,), (0,)), ((), ())),
                preferred_element_type=f32,
            )
            .astype(bf16)
            .reshape(tiles[1] - tiles[0], STRIP, share)
        )
        return slots_copies(
            xs,
            xr,
            group,
            tiles,
            (chunk * share, share),
            lambda j: x_s.at[group, chunk, j],
            lambda j: x_r.at[group, chunk, j],
        )

    def experts(group, tiles):
        count = tiles[1] - tiles[0]
        rows_in = xr[group, tiles[0] : tiles[1]].reshape(count * STRIP, width)
        gate_h = jnp.dot(rows_in, wg[...], preferred_element_type=f32)
        up_h = jnp.dot(rows_in, wu[...], preferred_element_type=f32)
        hidden = (gate_h * jax.nn.sigmoid(gate_h) * up_h).astype(bf16)
        fo[group, tiles[0] : tiles[1]] = (
            jnp.dot(hidden, wd[...], preferred_element_type=f32)
            .astype(bf16)
            .reshape(count, STRIP, width)
        )

    def give_part(group, tiles, chunk, no):
        return slots_copies(
            fo,
            rr,
            group,
            tiles,
            halves[chunk],
            lambda j: h_s.at[group, no, chunk, j],
            lambda j: h_r.at[group, no, chunk, j],
        )

    def combine(group, rows, tiles, cols):
        weights = jnp.where(hits(group, rows, tiles), table(group, 1, tiles), 0.0)
        high = weights.astype(bf16)
        low = (weights - high.astype(f32)).astype(bf16)
        at, size = cols
        back = rr[group, tiles[0] : tiles[1], :, at : at + size]
        back = back.reshape((tiles[1] - tiles[0]) * STRIP, size)
        return jnp.dot(high, back, preferred_element_type=f32) + jnp.dot(
            low, back, preferred_element_type=f32
        )

    every, later, side_tiles = (0, TILES), (0, LATE), ((0, 2), (1, 3))

    def reduced_copy(way, hop, no):
        cols = pl.ds(no * share, share)
        return remote(
            rs.at[way, hop, pl.ds(0, tokens), cols],
            rv.at[way, hop, pl.ds(0, tokens), cols],
            rs_s.at[way, hop, no],
            rs_r.at[way, hop, no],
            ahead[way],
        )

    def side_rows(side):
        return (side * tokens, (side + 1) * tokens)

    def own_term(way, hop):
        distance = hop + 1
        cols = halves[way]
        if distance == GROUPS:
            return combine(0, side_rows(1), later, cols)
        if distance < GROUPS:
            group, side = distance, way
        else:
            group, side = Z - distance, 1 - way
        return combine(group, side_rows(side), side_tiles[side], cols)

    def came(way, hop, no):
        return rv[way, hop, :, no * share : (no + 1) * share].astype(f32)

    def reduce_step(hop, coming):
        terms = [own_term(way, hop) for way in range(2)]
        passed = {}
        for no in range(2):
            for way in range(2):
                total = terms[way][:, no * share : (no + 1) * share]
                if hop:
                    coming[way, no].wait_recv()
                    total = total + came(way, hop - 1, no)
                rs[way, hop, :, no * share : (no + 1) * share] = total.astype(bf16)
                passed[way, no] = begin(reduced_copy(way, hop, no))
        return passed

    def give_first(group):
        return give_part(group, side_tiles[0], 0, 0) + give_part(group, side_tiles[1], 1, 0)

    def give_rest(group):
        return give_part(group, (2, 3), 0, 1) + give_part(group, (0, 1), 1, 1)

    dealt, given, rest = {}, {}, {}
    for step in range(1, GROUPS):
        passed = {}
        dealt[step] = []
        farthest = step == GROUPS - 1
        for chunk in range(PARTS):
            for way in range(2):
                arriving[way, chunk].wait_recv()
                if farthest and chunk % 2 != way:
                    continue
                src = ag.at[step, pl.ds(way * tokens, tokens), pl.ds(chunk * share, share)]
                group, side = (0, 1) if farthest else (step + 1, way)
                passed[way, chunk] = begin(gather_copy(src, group, side, chunk, way, step))
            dealt[step] += dispatch(step, chunk, every)
            if chunk == 1 and step > 1:
                finish(dealt[step - 1])
                experts(step - 1, every)
                given[step - 1] = give_first(step - 1)
            if chunk == PARTS - 1 and step == 1:
                finish(early)
                experts(0, (LATE, TILES))
        arriving = passed
    finish(given[1])
    coming = reduce_step(0, {})
    dealt[0] = []
    for chunk in range(PARTS):
        arriving[chunk % 2, chunk].wait_recv()
        dealt[0] += dispatch(0, chunk, later)
    last = GROUPS - 1
    finish(dealt[last])
    experts(last, every)
    given[last] = give_first(last)
    finish(given[2])
    coming = reduce_step(1, coming)
    finish(dealt[0])
    experts(0, later)
    given[0] = slots_copies(
        fo, rr, 0, later, whole, lambda j: b_s.at[j], lambda j: b_r.at[j]
    )
    for group in range(last, 0, -1):
        rest[group] = give_rest(group)
    given_early = slots_copies(
        fo, rr, 0, (LATE, TILES), whole, lambda j: l_s.at[j], lambda j: l_r.at[j]
    )
    finish(given[last])
    coming = reduce_step(2, coming)
    finish(given[0])
    coming = reduce_step(3, coming)
    for hop in range(GROUPS, HOPS):
        finish(rest[HOPS - hop])
        coming = reduce_step(hop, coming)
    finish(given_early)
    acc[...] += combine(0, side_rows(0), every, whole)
    for no in range(2):
        for way in range(2):
            coming[way, no].wait_recv()
            at = way * half + no * share
            acc[:, at : at + share] += came(way, HOPS - 1, no)

    branch = acc[...]
    factor = lax.rsqrt(jnp.mean(branch * branch, axis=1, keepdims=True) + epsilon)
    out[...] = (resid[...].astype(jnp.float32) + branch * factor * row_of(post_gain)).astype(
        jnp.bfloat16
    )
    for copy in started:
        copy.wait_send()


def body(
    x_in,
    gate_b,
    gate_c,
    conv_taps,
    out_proj,
    mix_gain,
    resid,
    pre_gain,
    expert_gate,
    expert_up,
    expert_down,
    shared_gate,
    shared_up,
    shared_down,
    post_gain,
    routes,
    route_weights,
):
    tokens, width = resid.shape
    rows, channels = x_in.shape
    hidden = expert_gate.shape[2]
    shared = shared_gate.shape[1]
    bf16, f32 = jnp.bfloat16, jnp.float32
    vmem = pl.BlockSpec(memory_space=pltpu.VMEM)
    hbm = pl.BlockSpec(memory_space=pl.ANY)
    dma = pltpu.SemaphoreType.DMA
    return pl.pallas_call(
        layer_kernel,
        out_shape=pltpu.VMEM((tokens, width), bf16),
        in_specs=[vmem] * 6 + [hbm] * 11,
        out_specs=vmem,
        scratch_shapes=[
            pltpu.VMEM((rows, channels), bf16),
            pltpu.VMEM((rows, channels), bf16),
            pltpu.VMEM((rows, channels), bf16),
            pltpu.VMEM((2, 8, channels), bf16),
            pltpu.VMEM((rows + 8, channels), f32),
            pltpu.VMEM((rows, channels), bf16),
            pltpu.VMEM((Y, tokens, channels), bf16),
            pltpu.VMEM((Y, channels, width), bf16),
            pltpu.VMEM((tokens, width), bf16),
            pltpu.VMEM((tokens, width), bf16),
            pltpu.VMEM((GROUPS, 2 * tokens, width), bf16),
            pltpu.VMEM((Z, 8, META), f32),
            pltpu.VMEM((Z, 8, META), f32),
            pltpu.VMEM((GROUPS, TILES, STRIP, width), bf16),
            pltpu.VMEM((GROUPS, TILES, STRIP, width), bf16),
            pltpu.VMEM((GROUPS, TILES, STRIP, width), bf16),
            pltpu.VMEM((GROUPS, TILES, STRIP, width), bf16),
            pltpu.VMEM((tokens, width), f32),
            pltpu.VMEM((2, HOPS, tokens, width // 2), bf16),
            pltpu.VMEM((2, HOPS, tokens, width // 2), bf16),
            pltpu.VMEM((tokens, width), f32),
            pltpu.VMEM((width, hidden), bf16),
            pltpu.VMEM((width, hidden), bf16),
            pltpu.VMEM((hidden, width), bf16),
            pltpu.VMEM((width, shared), bf16),
            pltpu.VMEM((width, shared), bf16),
            pltpu.VMEM((shared, width), bf16),
            dma((11,)),
            dma((2,)),
            dma((2,)),
            dma((2,)),
            dma((Y,)),
            dma((Y,)),
            dma((Y, SUBS)),
            dma((Y, SUBS)),
            dma((Y, SUBS)),
            dma((Y, SUBS)),
            dma((Y, 2, SUBS)),
            dma((Y, 2, SUBS)),
            dma((2, GROUPS, PARTS)),
            dma((2, GROUPS, PARTS)),
            dma((Z,)),
            dma((Z,)),
            dma((GROUPS, PARTS, PLANE)),
            dma((GROUPS, PARTS, PLANE)),
            dma((PLANE,)),
            dma((PLANE,)),
            dma((PLANE,)),
            dma((PLANE,)),
            dma((PLANE,)),
            dma((PLANE,)),
            dma((GROUPS, 2, 2, PLANE)),
            dma((GROUPS, 2, 2, PLANE)),
            dma((2, HOPS, 2)),
            dma((2, HOPS, 2)),
        ],
        compiler_params=pltpu.CompilerParams(
            collective_id=0, has_side_effects=True, vmem_limit_bytes=63 * 1024 * 1024
        ),
    )(
        conv_taps,
        mix_gain.reshape(-1, 128),
        pre_gain.reshape(-1, 128),
        post_gain.reshape(-1, 128),
        routes.T,
        route_weights.T,
        x_in,
        gate_b,
        gate_c,
        out_proj,
        resid,
        expert_gate[0],
        expert_up[0],
        expert_down[0],
        shared_gate,
        shared_up,
        shared_down,
    )


def solution(mesh):
    finer = Mesh(mesh.devices.reshape(Z, X, C, mesh.shape["tp"]), SP_TP)
    placed = (
        P(SP, "tp"),
        P(SP, "tp"),
        P(SP, "tp"),
        P(None, "tp"),
        P("tp", None),
        P(),
        P(SP_TP, None),
        P(),
        P(SP, None, None),
        P(SP, None, None),
        P(SP, None, None),
        P(),
        P(),
        P(),
        P(),
        P(SP_TP, None),
        P(SP_TP, None),
    )
    return jax.shard_map(
        body, mesh=finer, in_specs=placed, out_specs=P(SP_TP, None), check_vma=False
    )
```

```python
import jax
import jax.numpy as jnp
from jax import lax
from jax.experimental import pallas as pl
from jax.experimental.pallas import tpu as pltpu
from jax.sharding import Mesh
from jax.sharding import PartitionSpec as P

SP = ("sp_0", "sp_1", "sp_2")
SP_TP = ("sp_0", "sp_1", "sp_2", "tp")
MESH = pl.DeviceIdType.MESH

epsilon = 1e-06

Z, X, C, Y = 8, 4, 2, 4
PLANE = X * C
CAP = 12
SIDE = 2
ROWS = SIDE * CAP
SLOTS = PLANE * ROWS
GROUPS = Z // 2
META = 256
TILE = 8
TILES = ROWS // TILE
STRIP = PLANE * TILE
LATE = 2
PARTS = 4
HOPS = Z - 1
SUBS = 4


def row_of(ref):
    rows = ref[...].astype(jnp.float32)
    return jnp.concatenate([rows[i : i + 1] for i in range(rows.shape[0])], axis=1)


def fill_tables(meta, routes, route_weights):
    top, tokens = routes.shape
    f32, bf16 = jnp.float32, jnp.bfloat16
    experts = Z * PLANE
    expert = lax.broadcasted_iota(jnp.int32, (experts, tokens), 0)
    named = jnp.zeros((experts, tokens), f32)
    weight = jnp.zeros((experts, tokens), f32)
    for k in range(top):
        hot = expert == routes[k : k + 1]
        named = named + jnp.where(hot, 1.0, 0.0)
        weight = weight + jnp.where(hot, route_weights[k : k + 1], 0.0)
    named = named.T
    weight = weight.T
    row = lax.broadcasted_iota(jnp.int32, (tokens, tokens), 0)
    column = lax.broadcasted_iota(jnp.int32, (tokens, tokens), 1)
    below = jnp.where(row > column, 1.0, 0.0).astype(bf16)
    before = jnp.dot(below, named.astype(bf16), preferred_element_type=f32)
    place = jnp.where(named > 0.0, before, 100.0).astype(bf16)
    high = weight.astype(bf16)
    low = (weight - high.astype(f32)).astype(bf16)
    lane = lax.broadcasted_iota(jnp.int32, (experts, META), 1)
    expert = lax.broadcasted_iota(jnp.int32, (experts, META), 0)

    owner = (lane // TILE) % PLANE
    at = (lane // STRIP) * TILE + lane % TILE
    first = LATE * TILE
    spare = first - CAP
    own_at = jnp.where(at < first, at + TILE, at - first)
    far_at = jnp.where(at < first, at - spare, -1)
    token = lax.broadcasted_iota(jnp.int32, (tokens, META), 0).astype(f32) + 1.0
    z = lax.axis_index("sp_0")
    meta[...] = jnp.zeros_like(meta)
    for by in range(Z):
        side = 1 if by >= GROUPS else 0
        held = (far_at if side else own_at) if by % GROUPS == 0 else at - side * CAP
        within = held[0:1].astype(f32)
        spread = jnp.where(expert - owner == lax.rem(z + by, Z) * PLANE, 1.0, 0.0).astype(bf16)
        put = jnp.dot(place, spread, preferred_element_type=f32) == within
        tags = jnp.where(put, token + side * tokens, 0.0)
        weights = jnp.dot(high, spread, preferred_element_type=f32) + jnp.dot(
            low, spread, preferred_element_type=f32
        )
        meta[by, 0:1] = jnp.sum(tags, axis=0, keepdims=True)
        meta[by, 1:2] = jnp.sum(jnp.where(put, weights, 0.0), axis=0, keepdims=True)


def layer_kernel(
    taps,
    mix_gain,
    pre_gain,
    post_gain,
    routes,
    route_weights,
    x_hbm,
    gb_hbm,
    gc_hbm,
    proj_hbm,
    resid_hbm,
    wg_hbm,
    wu_hbm,
    wd_hbm,
    sg_hbm,
    su_hbm,
    sd_hbm,
    out,
    x_in,
    gb,
    gc,
    edge,
    mixed,
    conv,
    conv_in,
    proj,
    resid,
    normed,
    ag,
    meta,
    tables,
    xs,
    xr,
    fo,
    rr,
    part,
    rs,
    rv,
    acc,
    wg,
    wu,
    wd,
    sg,
    su,
    sd,
    load_sem,
    local_sem,
    edge_s,
    edge_r,
    conv_s,
    conv_r,
    wy_s,
    wy_r,
    wx_s,
    wx_r,
    wc_s,
    wc_r,
    ag_s,
    ag_r,
    meta_s,
    meta_r,
    x_s,
    x_r,
    e_s,
    e_r,
    b_s,
    b_r,
    l_s,
    l_r,
    h_s,
    h_r,
    rs_s,
    rs_r,
):
    z, x, c, y = (lax.axis_index(a) for a in SP_TP)
    me8 = x * C + c
    sp = z * PLANE + me8
    tokens, width = normed.shape
    half = width // 2
    share = width // PARTS

    def z_peer(by):
        return (lax.rem(z + by + Z, Z), x, c, y)

    def y_peer(by):
        return (z, x, c, lax.rem(y + by + Y, Y))

    def plane_peer(j):
        e = lax.rem(me8 + j, PLANE)
        return e, (z, e // C, lax.rem(e, C), y)

    def sp_peer(by):
        to = lax.rem(sp + by + Z * PLANE, Z * PLANE)
        return (to // PLANE, lax.rem(to, PLANE) // C, lax.rem(to, C), y)

    ahead = (z_peer(1), z_peer(-1))
    partner = (z, x, 1 - c, y)
    beside = (
        (z, lax.rem(x + 1, X), c, y),
        (z, lax.rem(x + X - 1, X), c, y),
        z_peer(1),
        z_peer(-1),
    )

    pairs = (
        (x_hbm, x_in),
        (gc_hbm, gc),
        (proj_hbm, proj.at[0]),
        (gb_hbm, gb),
        (resid_hbm, resid),
        (sg_hbm, sg),
        (su_hbm, su),
        (sd_hbm, sd),
        (wg_hbm, wg),
        (wu_hbm, wu),
        (wd_hbm, wd),
    )
    loads = [
        pltpu.make_async_copy(src, dst, load_sem.at[i]) for i, (src, dst) in enumerate(pairs)
    ]
    for load in loads:
        load.start()

    barrier = pltpu.get_barrier_semaphore()
    greeted = [z_peer(by) for by in range(1, Z)]
    greeted += [plane_peer(j)[1] for j in range(1, PLANE)]
    greeted += [y_peer(by) for by in range(1, Y)]
    greeted += [sp_peer(1), sp_peer(-1)]
    for device in greeted:
        pl.semaphore_signal(barrier, inc=1, device_id=device, device_id_type=MESH)
    fill_tables(meta, routes, route_weights)
    pl.semaphore_wait(barrier, len(greeted))

    def remote(src, dst, send, recv, device):
        return pltpu.make_async_remote_copy(
            src_ref=src,
            dst_ref=dst,
            send_sem=send,
            recv_sem=recv,
            device_id=device,
            device_id_type=MESH,
        )

    started = []

    def begin(copy):
        copy.start()
        started.append(copy)
        return copy

    count, channels = x_in.shape
    loads[0].wait()
    loads[1].wait()
    edges = [
        begin(
            remote(
                ref.at[pl.ds(count - 8, 8)], edge.at[i], edge_s.at[i], edge_r.at[i], sp_peer(1)
            )
        )
        for i, ref in enumerate((x_in, gc))
    ]

    unit = proj.shape[1] // (2 * C * SUBS)
    parity = lax.rem(x + z, 2)

    def unit_rows(core, par, sub):
        return pl.ds(pl.multiple_of(((core * 2 + par) * SUBS + sub) * unit, unit), unit)

    def y_unit(source, by, sub):
        way = 1 if (by == 1 or (by == 2 and sub < SUBS // 2)) else -1
        rows_at = unit_rows(c, parity, sub)
        return remote(
            proj.at[source, rows_at],
            proj.at[by, rows_at],
            wy_s.at[by, sub],
            wy_r.at[by, sub],
            y_peer(way),
        )

    loads[2].wait()
    units = {}
    near = [(by, (sub + (0 if by == 1 else 2)) % SUBS) for sub in range(SUBS) for by in (1, 3)]
    for by, sub in near:
        units[by, sub] = begin(y_unit(0, by, sub))

    loads[3].wait()
    mixed[8 : 8 + count] = gc[...].astype(jnp.float32) * x_in[...].astype(jnp.float32)
    reach = taps.shape[0] - 1
    tap = taps[...].astype(jnp.float32)
    mixed[0:8] = jnp.zeros((8, channels), jnp.float32)

    def convolve(first, last):
        total = None
        for index in range(reach + 1):
            at = 8 - reach + index
            term = tap[index : index + 1] * mixed[at + first : at + last]
            total = term if total is None else total + term
        conv[first:last] = (gb[first:last].astype(jnp.float32) * total).astype(jnp.bfloat16)

    convolve(0, count)

    def token_rows(owner):
        return pl.ds(pl.multiple_of(owner * tokens, tokens), tokens)

    def table_copy(by):
        group = by if by < GROUPS else (Z - by) % GROUPS
        slot = group * SIDE + (1 if by >= GROUPS else 0)
        return remote(meta.at[by], tables.at[slot], meta_s.at[by], meta_r.at[slot], z_peer(by))

    table_copies = [table_copy(by) for by in range(1, Z)]
    for copy in table_copies:
        copy.start()
    own_table = pltpu.make_async_copy(meta.at[0], tables.at[0], local_sem.at[1])
    own_table.start()

    def x_unit(by, sub):
        rows_at = unit_rows(c, parity, sub)
        return remote(
            proj.at[by, rows_at],
            proj.at[by, rows_at],
            wx_s.at[by, sub],
            wx_r.at[by, sub],
            beside[sub],
        )

    def core_unit(by, kind, sub):
        rows_at = unit_rows(c, parity if kind == 0 else 1 - parity, sub)
        return remote(
            proj.at[by, rows_at],
            proj.at[by, rows_at],
            wc_s.at[by, kind, sub],
            wc_r.at[by, kind, sub],
            partner,
        )

    def conv_copy(by):
        return remote(
            conv.at[token_rows(lax.rem(y + by, Y))],
            conv_in.at[by],
            conv_s.at[by],
            conv_r.at[by],
            y_peer(by),
        )

    conv_copies = []
    sides, swaps = {}, {}
    waiting = []

    def side_arrived(by, sub):
        sides[by, sub].wait_recv()
        swaps[by, 1, sub] = begin(core_unit(by, 1, sub))

    relayed = {(1, 0), (1, 1), (3, 2), (3, 3)}
    for by, sub in near + [(2, 0), (2, 2), (2, 1), (2, 3)]:
        units[by, sub].wait_recv()
        if (by, sub) in relayed:
            units[2, sub] = begin(y_unit(by, 2, sub))
        sides[by, sub] = begin(x_unit(by, sub))
        swaps[by, 0, sub] = begin(core_unit(by, 0, sub))
        waiting.append((by, sub))
        if (by, sub) == (3, 3):
            for copy in edges:
                copy.wait_recv()
            before = edge[1].astype(jnp.float32) * edge[0].astype(jnp.float32)
            mixed[0:8] = jnp.where(sp > 0, before, 0.0)
            convolve(0, 8)
            for to in range(1, Y):
                conv_copies.append(begin(conv_copy(to)))
        if len(waiting) > 4:
            side_arrived(*waiting.pop(0))
    part[0:tokens] = jnp.dot(conv[token_rows(y)], proj[0], preferred_element_type=jnp.float32)
    for by, sub in waiting:
        side_arrived(by, sub)
    for by in (1, 3, 2):
        conv_copies[by - 1].wait_recv()
        for kind in range(2):
            for sub in range(SUBS):
                swaps[by, kind, sub].wait_recv()
        part[0:tokens] += jnp.dot(conv_in[by], proj[by], preferred_element_type=jnp.float32)
    projected = part[0:tokens]
    loads[4].wait()
    row_scale = lax.rsqrt(jnp.mean(projected * projected, axis=1, keepdims=True) + epsilon)
    resid1 = (resid[...].astype(jnp.float32) + projected * row_scale * row_of(mix_gain)).astype(
        jnp.bfloat16
    )
    resid[...] = resid1
    wide_resid = resid1.astype(jnp.float32)
    normed[...] = (
        wide_resid
        * lax.rsqrt(jnp.mean(wide_resid * wide_resid, axis=1, keepdims=True) + epsilon)
        * row_of(pre_gain)
    ).astype(jnp.bfloat16)

    def gather_copy(src, group, side, chunk, way, step):
        return remote(
            src,
            ag.at[group, pl.ds(side * tokens, tokens), pl.ds(chunk * share, share)],
            ag_s.at[way, step, chunk],
            ag_r.at[way, step, chunk],
            ahead[way],
        )

    arriving = {}
    for chunk in range(PARTS):
        for way in range(2):
            src = normed.at[pl.ds(0, tokens), pl.ds(chunk * share, share)]
            arriving[way, chunk] = begin(gather_copy(src, 1, way, chunk, way, 0))
    own_rows = pltpu.make_async_copy(normed, ag.at[0, pl.ds(0, tokens)], local_sem.at[0])
    own_rows.start()

    def aligned(at):
        return at if isinstance(at, int) else pl.multiple_of(at, share)

    def slots_copies(src, dst, group, tiles, cols, send, recv):
        def view(ref, e):
            strip = pl.ds(pl.multiple_of(e * TILE, TILE), TILE)
            lanes = pl.ds(aligned(cols[0]), cols[1])
            return ref.at[group, pl.ds(tiles[0], tiles[1] - tiles[0]), strip, lanes]

        copies = []
        for j in range(1, PLANE):
            e, device = plane_peer(j)
            copies.append(remote(view(src, e), view(dst, me8), send(j), recv(j), device))
        copies.append(pltpu.make_async_copy(view(src, me8), view(dst, me8), send(0)))
        for copy in copies:
            copy.start()
        return copies

    whole = (0, width)

    def finish(copies):
        for copy in copies:
            copy.wait()

    f32, bf16 = jnp.float32, jnp.bfloat16
    late_rows = LATE * STRIP

    own_table.wait()
    token = lax.broadcasted_iota(jnp.int32, (tokens, SLOTS - late_rows), 0).astype(f32)
    chosen = jnp.where(token + 1.0 == tables[0, 0:1, late_rows:SLOTS], 1.0, 0.0).astype(bf16)
    xs[0, LATE] = lax.dot_general(
        chosen, normed[...], (((0,), (0,)), ((), ())), preferred_element_type=f32
    ).astype(bf16)
    early = slots_copies(
        xs, xr, 0, (LATE, TILES), whole, lambda j: e_s.at[j], lambda j: e_r.at[j]
    )

    for load in loads[5:8]:
        load.wait()
    rows = normed[...]
    shared_g = jnp.dot(rows, sg[...], preferred_element_type=f32)
    shared_u = jnp.dot(rows, su[...], preferred_element_type=f32)
    shared_h = (shared_g * jax.nn.sigmoid(shared_g) * shared_u).astype(bf16)
    acc[...] = jnp.dot(shared_h, sd[...], preferred_element_type=f32)
    for load in loads[8:]:
        load.wait()
    own_rows.wait()
    finish(table_copies)

    def table(group, row, tiles):
        both = tables[2 * group] + tables[2 * group + 1]
        if tiles[0]:
            both = pltpu.roll(both, META - tiles[0] * STRIP, 1)
        return both[row : row + 1, 0 : (tiles[1] - tiles[0]) * STRIP]

    def hits(group, rows, tiles):
        first, last = rows
        shape = (last - first, (tiles[1] - tiles[0]) * STRIP)
        row = lax.broadcasted_iota(jnp.int32, shape, 0).astype(f32)
        return row + (first + 1.0) == table(group, 0, tiles)

    def dispatch(group, chunk, tiles):
        picks = jnp.where(hits(group, (0, 2 * tokens), tiles), 1.0, 0.0).astype(bf16)
        cols = slice(chunk * share, (chunk + 1) * share)
        xs[group, tiles[0] : tiles[1], :, cols] = (
            lax.dot_general(
                picks,
                ag[group, :, cols],
                (((0,), (0,)), ((), ())),
                preferred_element_type=f32,
            )
            .astype(bf16)
            .reshape(tiles[1] - tiles[0], STRIP, share)
        )
        return slots_copies(
            xs,
            xr,
            group,
            tiles,
            (chunk * share, share),
            lambda j: x_s.at[group, chunk, j],
            lambda j: x_r.at[group, chunk, j],
        )

    def experts(group, tiles):
        count = tiles[1] - tiles[0]
        rows_in = xr[group, tiles[0] : tiles[1]].reshape(count * STRIP, width)
        gate_h = jnp.dot(rows_in, wg[...], preferred_element_type=f32)
        up_h = jnp.dot(rows_in, wu[...], preferred_element_type=f32)
        hidden = (gate_h * jax.nn.sigmoid(gate_h) * up_h).astype(bf16)
        fo[group, tiles[0] : tiles[1]] = (
            jnp.dot(hidden, wd[...], preferred_element_type=f32)
            .astype(bf16)
            .reshape(count, STRIP, width)
        )

    def give_part(group, tiles, cols, turn, no):
        return slots_copies(
            fo,
            rr,
            group,
            tiles,
            cols,
            lambda j: h_s.at[group, turn, no, j],
            lambda j: h_r.at[group, turn, no, j],
        )

    def combine(group, rows, tiles, cols):
        weights = jnp.where(hits(group, rows, tiles), table(group, 1, tiles), 0.0)
        high = weights.astype(bf16)
        low = (weights - high.astype(f32)).astype(bf16)
        at, size = cols
        back = rr[group, tiles[0] : tiles[1], :, pl.ds(aligned(at), size)]
        back = back.reshape((tiles[1] - tiles[0]) * STRIP, size)
        return jnp.dot(high, back, preferred_element_type=f32) + jnp.dot(
            low, back, preferred_element_type=f32
        )

    every, later, side_tiles = (0, TILES), (0, LATE), ((0, 2), (1, 3))

    def half_of(way, by):
        turned = (lax.rem(z + by + Z, Z) // 2) % 2
        return (turned if way == 0 else 1 - turned) * half

    def reduced_copy(way, hop, no):
        cols = pl.ds(no * share, share)
        return remote(
            rs.at[way, hop, pl.ds(0, tokens), cols],
            rv.at[way, hop, pl.ds(0, tokens), cols],
            rs_s.at[way, hop, no],
            rs_r.at[way, hop, no],
            ahead[way],
        )

    def side_rows(side):
        return (side * tokens, (side + 1) * tokens)

    def own_term(way, hop, no):
        distance = hop + 1
        owner = distance if way else -distance
        cols = (half_of(way, owner) + no * share, share)
        if distance == GROUPS:
            return combine(0, side_rows(1), later, cols)
        if distance < GROUPS:
            group, side = distance, way
        else:
            group, side = Z - distance, 1 - way
        return combine(group, side_rows(side), side_tiles[side], cols)

    def came(way, hop, no):
        return rv[way, hop, :, no * share : (no + 1) * share].astype(f32)

    def reduce_step(hop, coming, ready):
        passed = {}
        for no in range(2):
            finish(ready[no])
            for way in range(2):
                total = own_term(way, hop, no)
                if hop:
                    coming[way, no].wait_recv()
                    total = total + came(way, hop - 1, no)
                rs[way, hop, :, no * share : (no + 1) * share] = total.astype(bf16)
                passed[way, no] = begin(reduced_copy(way, hop, no))
        return passed

    def give_first(group):
        left = half_of(0, -group)
        copies = []
        for no in range(2):
            cols = (left + no * share, share)
            if group % 2:
                copies.append(give_part(group, every, cols, no, 0))
            else:
                other = (half - left + no * share, share)
                copies.append(
                    give_part(group, side_tiles[0], cols, no, 0)
                    + give_part(group, side_tiles[1], other, no, 1)
                )
        return copies

    def give_rest(group):
        left = half_of(0, -group)
        if group % 2:
            return give_part(group, every, (half - left, half), 2, 0)
        return give_part(group, (2, 3), (left, half), 2, 0) + give_part(
            group, (0, 1), (half - left, half), 2, 1
        )

    def give_late(no):
        copies = []
        for side in range(2):
            copies += slots_copies(
                fo,
                rr,
                0,
                later,
                (side * half + no * share, share),
                lambda j: b_s.at[no, side, j],
                lambda j: b_r.at[no, side, j],
            )
        return copies

    dealt, given, rest = {}, {}, {}
    for step in range(1, GROUPS):
        passed = {}
        dealt[step] = []
        farthest = step == GROUPS - 1
        for chunk in range(PARTS):
            for way in range(2):
                arriving[way, chunk].wait_recv()
                if farthest and chunk % 2 != way:
                    continue
                src = ag.at[step, pl.ds(way * tokens, tokens), pl.ds(chunk * share, share)]
                group, side = (0, 1) if farthest else (step + 1, way)
                passed[way, chunk] = begin(gather_copy(src, group, side, chunk, way, step))
            dealt[step] += dispatch(step, chunk, every)
            if chunk == step - 1 and step > 1:
                finish(dealt[step - 1])
                experts(step - 1, every)
                given[step - 1] = give_first(step - 1)
            if chunk == PARTS - 1 and step == 1:
                finish(early)
                experts(0, (LATE, TILES))
        arriving = passed
    coming = reduce_step(0, {}, given[1])
    dealt[0] = []
    for chunk in range(PARTS):
        arriving[chunk % 2, chunk].wait_recv()
        dealt[0] += dispatch(0, chunk, later)
    last = GROUPS - 1
    finish(dealt[last])
    experts(last, every)
    given[last] = give_first(last)
    coming = reduce_step(1, coming, given[2])
    finish(dealt[0])
    experts(0, later)
    given[0] = [give_late(no) for no in range(2)]
    for group in range(last, 0, -1):
        rest[group] = give_rest(group)
    given_early = slots_copies(
        fo, rr, 0, (LATE, TILES), whole, lambda j: l_s.at[j], lambda j: l_r.at[j]
    )
    coming = reduce_step(2, coming, given[last])
    coming = reduce_step(3, coming, given[0])
    for hop in range(GROUPS, HOPS):
        coming = reduce_step(hop, coming, (rest[HOPS - hop], ()))
    finish(given_early)
    acc[...] += combine(0, side_rows(0), every, whole)
    for no in range(2):
        for way in range(2):
            coming[way, no].wait_recv()
            cols = pl.ds(aligned(half_of(way, 0) + no * share), share)
            acc[:, cols] += came(way, HOPS - 1, no)

    branch = acc[...]
    factor = lax.rsqrt(jnp.mean(branch * branch, axis=1, keepdims=True) + epsilon)
    out[...] = (resid[...].astype(jnp.float32) + branch * factor * row_of(post_gain)).astype(
        jnp.bfloat16
    )
    for copy in started:
        copy.wait_send()


def body(
    x_in,
    gate_b,
    gate_c,
    conv_taps,
    out_proj,
    mix_gain,
    resid,
    pre_gain,
    expert_gate,
    expert_up,
    expert_down,
    shared_gate,
    shared_up,
    shared_down,
    post_gain,
    routes,
    route_weights,
):
    tokens, width = resid.shape
    rows, channels = x_in.shape
    hidden = expert_gate.shape[2]
    shared = shared_gate.shape[1]
    bf16, f32 = jnp.bfloat16, jnp.float32
    vmem = pl.BlockSpec(memory_space=pltpu.VMEM)
    hbm = pl.BlockSpec(memory_space=pl.ANY)
    dma = pltpu.SemaphoreType.DMA
    return pl.pallas_call(
        layer_kernel,
        out_shape=pltpu.VMEM((tokens, width), bf16),
        in_specs=[vmem] * 6 + [hbm] * 11,
        out_specs=vmem,
        scratch_shapes=[
            pltpu.VMEM((rows, channels), bf16),
            pltpu.VMEM((rows, channels), bf16),
            pltpu.VMEM((rows, channels), bf16),
            pltpu.VMEM((2, 8, channels), bf16),
            pltpu.VMEM((rows + 8, channels), f32),
            pltpu.VMEM((rows, channels), bf16),
            pltpu.VMEM((Y, tokens, channels), bf16),
            pltpu.VMEM((Y, channels, width), bf16),
            pltpu.VMEM((tokens, width), bf16),
            pltpu.VMEM((tokens, width), bf16),
            pltpu.VMEM((GROUPS, 2 * tokens, width), bf16),
            pltpu.VMEM((Z, 8, META), f32),
            pltpu.VMEM((Z, 8, META), f32),
            pltpu.VMEM((GROUPS, TILES, STRIP, width), bf16),
            pltpu.VMEM((GROUPS, TILES, STRIP, width), bf16),
            pltpu.VMEM((GROUPS, TILES, STRIP, width), bf16),
            pltpu.VMEM((GROUPS, TILES, STRIP, width), bf16),
            pltpu.VMEM((tokens, width), f32),
            pltpu.VMEM((2, HOPS, tokens, width // 2), bf16),
            pltpu.VMEM((2, HOPS, tokens, width // 2), bf16),
            pltpu.VMEM((tokens, width), f32),
            pltpu.VMEM((width, hidden), bf16),
            pltpu.VMEM((width, hidden), bf16),
            pltpu.VMEM((hidden, width), bf16),
            pltpu.VMEM((width, shared), bf16),
            pltpu.VMEM((width, shared), bf16),
            pltpu.VMEM((shared, width), bf16),
            dma((11,)),
            dma((2,)),
            dma((2,)),
            dma((2,)),
            dma((Y,)),
            dma((Y,)),
            dma((Y, SUBS)),
            dma((Y, SUBS)),
            dma((Y, SUBS)),
            dma((Y, SUBS)),
            dma((Y, 2, SUBS)),
            dma((Y, 2, SUBS)),
            dma((2, GROUPS, PARTS)),
            dma((2, GROUPS, PARTS)),
            dma((Z,)),
            dma((Z,)),
            dma((GROUPS, PARTS, PLANE)),
            dma((GROUPS, PARTS, PLANE)),
            dma((PLANE,)),
            dma((PLANE,)),
            dma((2, 2, PLANE)),
            dma((2, 2, PLANE)),
            dma((PLANE,)),
            dma((PLANE,)),
            dma((GROUPS, 3, 2, PLANE)),
            dma((GROUPS, 3, 2, PLANE)),
            dma((2, HOPS, 2)),
            dma((2, HOPS, 2)),
        ],
        compiler_params=pltpu.CompilerParams(
            collective_id=0, has_side_effects=True, vmem_limit_bytes=63 * 1024 * 1024
        ),
    )(
        conv_taps,
        mix_gain.reshape(-1, 128),
        pre_gain.reshape(-1, 128),
        post_gain.reshape(-1, 128),
        routes.T,
        route_weights.T,
        x_in,
        gate_b,
        gate_c,
        out_proj,
        resid,
        expert_gate[0],
        expert_up[0],
        expert_down[0],
        shared_gate,
        shared_up,
        shared_down,
    )


def solution(mesh):
    finer = Mesh(mesh.devices.reshape(Z, X, C, mesh.shape["tp"]), SP_TP)
    placed = (
        P(SP, "tp"),
        P(SP, "tp"),
        P(SP, "tp"),
        P(None, "tp"),
        P("tp", None),
        P(),
        P(SP_TP, None),
        P(),
        P(SP, None, None),
        P(SP, None, None),
        P(SP, None, None),
        P(),
        P(),
        P(),
        P(),
        P(SP_TP, None),
        P(SP_TP, None),
    )
    return jax.shard_map(
        body, mesh=finer, in_specs=placed, out_specs=P(SP_TP, None), check_vma=False
    )
```

```python
import jax
import jax.numpy as jnp
from jax import lax
from jax.experimental import pallas as pl
from jax.experimental.pallas import tpu as pltpu
from jax.sharding import Mesh
from jax.sharding import PartitionSpec as P

SP = ("sp_0", "sp_1", "sp_2")
SP_TP = ("sp_0", "sp_1", "sp_2", "tp")
MESH = pl.DeviceIdType.MESH

epsilon = 1e-06

Z, X, C, Y = 8, 4, 2, 4
PLANE = X * C
CAP = 12
SIDE = 2
ROWS = SIDE * CAP
SLOTS = PLANE * ROWS
GROUPS = Z // 2
META = 256
TILE = 8
TILES = ROWS // TILE
STRIP = PLANE * TILE
LATE = 2
PARTS = 4
HOPS = Z - 1
SUBS = 4


def row_of(ref):
    rows = ref[...].astype(jnp.float32)
    return jnp.concatenate([rows[i : i + 1] for i in range(rows.shape[0])], axis=1)


def fill_tables(meta, routes, route_weights):
    top, tokens = routes.shape
    f32, bf16 = jnp.float32, jnp.bfloat16
    experts = Z * PLANE
    expert = lax.broadcasted_iota(jnp.int32, (experts, tokens), 0)
    named = jnp.zeros((experts, tokens), f32)
    weight = jnp.zeros((experts, tokens), f32)
    for k in range(top):
        hot = expert == routes[k : k + 1]
        named = named + jnp.where(hot, 1.0, 0.0)
        weight = weight + jnp.where(hot, route_weights[k : k + 1], 0.0)
    named = named.T
    weight = weight.T
    row = lax.broadcasted_iota(jnp.int32, (tokens, tokens), 0)
    column = lax.broadcasted_iota(jnp.int32, (tokens, tokens), 1)
    below = jnp.where(row > column, 1.0, 0.0).astype(bf16)
    before = jnp.dot(below, named.astype(bf16), preferred_element_type=f32)
    place = jnp.where(named > 0.0, before, 100.0).astype(bf16)
    high = weight.astype(bf16)
    low = (weight - high.astype(f32)).astype(bf16)
    lane = lax.broadcasted_iota(jnp.int32, (experts, META), 1)
    expert = lax.broadcasted_iota(jnp.int32, (experts, META), 0)

    owner = (lane // TILE) % PLANE
    at = (lane // STRIP) * TILE + lane % TILE
    first = LATE * TILE
    spare = first - CAP
    own_at = jnp.where(at < first, at + TILE, at - first)
    far_at = jnp.where(at < first, at - spare, -1)
    token = lax.broadcasted_iota(jnp.int32, (tokens, META), 0).astype(f32) + 1.0
    z = lax.axis_index("sp_0")
    meta[...] = jnp.zeros_like(meta)
    for by in range(Z):
        side = 1 if by >= GROUPS else 0
        held = (far_at if side else own_at) if by % GROUPS == 0 else at - side * CAP
        within = held[0:1].astype(f32)
        spread = jnp.where(expert - owner == lax.rem(z + by, Z) * PLANE, 1.0, 0.0).astype(bf16)
        put = jnp.dot(place, spread, preferred_element_type=f32) == within
        tags = jnp.where(put, token + side * tokens, 0.0)
        weights = jnp.dot(high, spread, preferred_element_type=f32) + jnp.dot(
            low, spread, preferred_element_type=f32
        )
        meta[by, 0:1] = jnp.sum(tags, axis=0, keepdims=True)
        meta[by, 1:2] = jnp.sum(jnp.where(put, weights, 0.0), axis=0, keepdims=True)


def layer_kernel(
    taps_hbm,
    mix_hbm,
    pre_hbm,
    post_hbm,
    routes_hbm,
    route_weights_hbm,
    x_hbm,
    gb_hbm,
    gc_hbm,
    proj_hbm,
    resid_hbm,
    wg_hbm,
    wu_hbm,
    wd_hbm,
    sg_hbm,
    su_hbm,
    sd_hbm,
    out,
    taps,
    mix_gain,
    pre_gain,
    post_gain,
    routes,
    route_weights,
    x_in,
    gb,
    gc,
    edge,
    mixed,
    conv,
    conv_in,
    proj,
    resid,
    normed,
    ag,
    meta,
    tables,
    xs,
    xr,
    fo,
    rr,
    part,
    rs,
    rv,
    acc,
    wg,
    wu,
    wd,
    sg,
    su,
    sd,
    load_sem,
    local_sem,
    edge_s,
    edge_r,
    conv_s,
    conv_r,
    wy_s,
    wy_r,
    wx_s,
    wx_r,
    wc_s,
    wc_r,
    ag_s,
    ag_r,
    meta_s,
    meta_r,
    x_s,
    x_r,
    e_s,
    e_r,
    b_s,
    b_r,
    l_s,
    l_r,
    h_s,
    h_r,
    rs_s,
    rs_r,
):
    z, x, c, y = (lax.axis_index(a) for a in SP_TP)
    me8 = x * C + c
    sp = z * PLANE + me8
    tokens, width = normed.shape
    half = width // 2
    share = width // PARTS

    def z_peer(by):
        return (lax.rem(z + by + Z, Z), x, c, y)

    def y_peer(by):
        return (z, x, c, lax.rem(y + by + Y, Y))

    def plane_peer(j):
        e = lax.rem(me8 + j, PLANE)
        return e, (z, e // C, lax.rem(e, C), y)

    def sp_peer(by):
        to = lax.rem(sp + by + Z * PLANE, Z * PLANE)
        return (to // PLANE, lax.rem(to, PLANE) // C, lax.rem(to, C), y)

    ahead = (z_peer(1), z_peer(-1))
    partner = (z, x, 1 - c, y)
    beside = (
        (z, lax.rem(x + 1, X), c, y),
        (z, lax.rem(x + X - 1, X), c, y),
        z_peer(1),
        z_peer(-1),
    )

    pairs = (
        (x_hbm, x_in),
        (gc_hbm, gc),
        (proj_hbm, proj.at[0]),
        (gb_hbm, gb),
        (resid_hbm, resid),
        (sg_hbm, sg),
        (su_hbm, su),
        (sd_hbm, sd),
        (wg_hbm, wg),
        (wu_hbm, wu),
        (wd_hbm, wd),
    )
    small = (
        (routes_hbm, routes),
        (route_weights_hbm, route_weights),
        (taps_hbm, taps),
        (mix_hbm, mix_gain),
        (pre_hbm, pre_gain),
        (post_hbm, post_gain),
    )
    barrier = pltpu.get_barrier_semaphore()
    greeted = [z_peer(by) for by in range(1, Z)]
    greeted += [plane_peer(j)[1] for j in range(1, PLANE)]
    greeted += [y_peer(by) for by in range(1, Y)]
    greeted += [sp_peer(1), sp_peer(-1)]
    for device in greeted:
        pl.semaphore_signal(barrier, inc=1, device_id=device, device_id_type=MESH)
    loads = [
        pltpu.make_async_copy(src, dst, load_sem.at[i])
        for i, (src, dst) in enumerate(pairs + small)
    ]
    few = loads[len(pairs) :]
    loads = loads[: len(pairs)]
    for load in few:
        load.start()
    for load in loads:
        load.start()

    few[0].wait()
    few[1].wait()
    fill_tables(meta, routes, route_weights)
    pl.semaphore_wait(barrier, len(greeted))
    for load in few[2:]:
        load.wait()

    def remote(src, dst, send, recv, device):
        return pltpu.make_async_remote_copy(
            src_ref=src,
            dst_ref=dst,
            send_sem=send,
            recv_sem=recv,
            device_id=device,
            device_id_type=MESH,
        )

    started = []

    def begin(copy):
        copy.start()
        started.append(copy)
        return copy

    count, channels = x_in.shape
    loads[0].wait()
    loads[1].wait()
    edges = [
        begin(
            remote(
                ref.at[pl.ds(count - 8, 8)], edge.at[i], edge_s.at[i], edge_r.at[i], sp_peer(1)
            )
        )
        for i, ref in enumerate((x_in, gc))
    ]

    unit = proj.shape[1] // (2 * C * SUBS)
    parity = lax.rem(x + z, 2)

    def unit_rows(core, par, sub):
        return pl.ds(pl.multiple_of(((core * 2 + par) * SUBS + sub) * unit, unit), unit)

    def y_unit(source, by, sub):
        way = 1 if (by == 1 or (by == 2 and sub < SUBS // 2)) else -1
        rows_at = unit_rows(c, parity, sub)
        return remote(
            proj.at[source, rows_at],
            proj.at[by, rows_at],
            wy_s.at[by, sub],
            wy_r.at[by, sub],
            y_peer(way),
        )

    loads[2].wait()
    units = {}
    near = [(by, (sub + (0 if by == 1 else 2)) % SUBS) for sub in range(SUBS) for by in (1, 3)]
    for by, sub in near:
        units[by, sub] = begin(y_unit(0, by, sub))

    loads[3].wait()
    mixed[8 : 8 + count] = gc[...].astype(jnp.float32) * x_in[...].astype(jnp.float32)
    reach = taps.shape[0] - 1
    tap = taps[...].astype(jnp.float32)
    mixed[0:8] = jnp.zeros((8, channels), jnp.float32)

    def convolve(first, last):
        total = None
        for index in range(reach + 1):
            at = 8 - reach + index
            term = tap[index : index + 1] * mixed[at + first : at + last]
            total = term if total is None else total + term
        conv[first:last] = (gb[first:last].astype(jnp.float32) * total).astype(jnp.bfloat16)

    convolve(0, count)

    def token_rows(owner):
        return pl.ds(pl.multiple_of(owner * tokens, tokens), tokens)

    def table_copy(by):
        group = by if by < GROUPS else (Z - by) % GROUPS
        slot = group * SIDE + (1 if by >= GROUPS else 0)
        return remote(meta.at[by], tables.at[slot], meta_s.at[by], meta_r.at[slot], z_peer(by))

    table_copies = [table_copy(by) for by in range(1, Z)]
    for copy in table_copies:
        copy.start()
    own_table = pltpu.make_async_copy(meta.at[0], tables.at[0], local_sem.at[1])
    own_table.start()

    def x_unit(by, sub):
        rows_at = unit_rows(c, parity, sub)
        return remote(
            proj.at[by, rows_at],
            proj.at[by, rows_at],
            wx_s.at[by, sub],
            wx_r.at[by, sub],
            beside[sub],
        )

    def core_unit(by, kind, sub):
        rows_at = unit_rows(c, parity if kind == 0 else 1 - parity, sub)
        return remote(
            proj.at[by, rows_at],
            proj.at[by, rows_at],
            wc_s.at[by, kind, sub],
            wc_r.at[by, kind, sub],
            partner,
        )

    def conv_copy(by):
        return remote(
            conv.at[token_rows(lax.rem(y + by, Y))],
            conv_in.at[by],
            conv_s.at[by],
            conv_r.at[by],
            y_peer(by),
        )

    conv_copies = []
    sides, swaps = {}, {}
    waiting = []

    def side_arrived(by, sub):
        sides[by, sub].wait_recv()
        swaps[by, 1, sub] = begin(core_unit(by, 1, sub))

    relayed = {(1, 0), (1, 1), (3, 2), (3, 3)}
    for by, sub in near + [(2, 0), (2, 2), (2, 1), (2, 3)]:
        units[by, sub].wait_recv()
        if (by, sub) in relayed:
            units[2, sub] = begin(y_unit(by, 2, sub))
        sides[by, sub] = begin(x_unit(by, sub))
        swaps[by, 0, sub] = begin(core_unit(by, 0, sub))
        waiting.append((by, sub))
        if (by, sub) == (3, 3):
            for copy in edges:
                copy.wait_recv()
            before = edge[1].astype(jnp.float32) * edge[0].astype(jnp.float32)
            mixed[0:8] = jnp.where(sp > 0, before, 0.0)
            convolve(0, 8)
            for to in range(1, Y):
                conv_copies.append(begin(conv_copy(to)))
        if len(waiting) > 4:
            side_arrived(*waiting.pop(0))
    part[0:tokens] = jnp.dot(conv[token_rows(y)], proj[0], preferred_element_type=jnp.float32)
    for by, sub in waiting:
        side_arrived(by, sub)
    for by in (1, 3, 2):
        conv_copies[by - 1].wait_recv()
        for kind in range(2):
            for sub in range(SUBS):
                swaps[by, kind, sub].wait_recv()
        part[0:tokens] += jnp.dot(conv_in[by], proj[by], preferred_element_type=jnp.float32)
    projected = part[0:tokens]
    loads[4].wait()
    row_scale = lax.rsqrt(jnp.mean(projected * projected, axis=1, keepdims=True) + epsilon)
    resid1 = (resid[...].astype(jnp.float32) + projected * row_scale * row_of(mix_gain)).astype(
        jnp.bfloat16
    )
    resid[...] = resid1
    wide_resid = resid1.astype(jnp.float32)
    normed[...] = (
        wide_resid
        * lax.rsqrt(jnp.mean(wide_resid * wide_resid, axis=1, keepdims=True) + epsilon)
        * row_of(pre_gain)
    ).astype(jnp.bfloat16)

    def gather_copy(src, group, side, chunk, way, step):
        return remote(
            src,
            ag.at[group, pl.ds(side * tokens, tokens), pl.ds(chunk * share, share)],
            ag_s.at[way, step, chunk],
            ag_r.at[way, step, chunk],
            ahead[way],
        )

    arriving = {}
    for chunk in range(PARTS):
        for way in range(2):
            src = normed.at[pl.ds(0, tokens), pl.ds(chunk * share, share)]
            arriving[way, chunk] = begin(gather_copy(src, 1, way, chunk, way, 0))
    own_rows = pltpu.make_async_copy(normed, ag.at[0, pl.ds(0, tokens)], local_sem.at[0])
    own_rows.start()

    def aligned(at):
        return at if isinstance(at, int) else pl.multiple_of(at, share)

    def slots_copies(src, dst, group, tiles, cols, send, recv):
        def view(ref, e):
            strip = pl.ds(pl.multiple_of(e * TILE, TILE), TILE)
            lanes = pl.ds(aligned(cols[0]), cols[1])
            return ref.at[group, pl.ds(tiles[0], tiles[1] - tiles[0]), strip, lanes]

        copies = []
        for j in range(1, PLANE):
            e, device = plane_peer(j)
            copies.append(remote(view(src, e), view(dst, me8), send(j), recv(j), device))
        copies.append(pltpu.make_async_copy(view(src, me8), view(dst, me8), send(0)))
        for copy in copies:
            copy.start()
        return copies

    whole = (0, width)

    def finish(copies):
        for copy in copies:
            copy.wait()

    f32, bf16 = jnp.float32, jnp.bfloat16
    late_rows = LATE * STRIP

    own_table.wait()
    token = lax.broadcasted_iota(jnp.int32, (tokens, SLOTS - late_rows), 0).astype(f32)
    chosen = jnp.where(token + 1.0 == tables[0, 0:1, late_rows:SLOTS], 1.0, 0.0).astype(bf16)
    xs[0, LATE] = lax.dot_general(
        chosen, normed[...], (((0,), (0,)), ((), ())), preferred_element_type=f32
    ).astype(bf16)
    early = slots_copies(
        xs, xr, 0, (LATE, TILES), whole, lambda j: e_s.at[j], lambda j: e_r.at[j]
    )

    for load in loads[5:8]:
        load.wait()
    rows = normed[...]
    shared_g = jnp.dot(rows, sg[...], preferred_element_type=f32)
    shared_u = jnp.dot(rows, su[...], preferred_element_type=f32)
    shared_h = (shared_g * jax.nn.sigmoid(shared_g) * shared_u).astype(bf16)
    acc[...] = jnp.dot(shared_h, sd[...], preferred_element_type=f32)
    for load in loads[8:]:
        load.wait()
    own_rows.wait()
    finish(table_copies)

    def table(group, row, tiles):
        both = tables[2 * group] + tables[2 * group + 1]
        if tiles[0]:
            both = pltpu.roll(both, META - tiles[0] * STRIP, 1)
        return both[row : row + 1, 0 : (tiles[1] - tiles[0]) * STRIP]

    def hits(group, rows, tiles):
        first, last = rows
        shape = (last - first, (tiles[1] - tiles[0]) * STRIP)
        row = lax.broadcasted_iota(jnp.int32, shape, 0).astype(f32)
        return row + (first + 1.0) == table(group, 0, tiles)

    def dispatch(group, chunk, tiles):
        picks = jnp.where(hits(group, (0, 2 * tokens), tiles), 1.0, 0.0).astype(bf16)
        cols = slice(chunk * share, (chunk + 1) * share)
        xs[group, tiles[0] : tiles[1], :, cols] = (
            lax.dot_general(
                picks,
                ag[group, :, cols],
                (((0,), (0,)), ((), ())),
                preferred_element_type=f32,
            )
            .astype(bf16)
            .reshape(tiles[1] - tiles[0], STRIP, share)
        )
        return slots_copies(
            xs,
            xr,
            group,
            tiles,
            (chunk * share, share),
            lambda j: x_s.at[group, chunk, j],
            lambda j: x_r.at[group, chunk, j],
        )

    def experts(group, tiles):
        count = tiles[1] - tiles[0]
        rows_in = xr[group, tiles[0] : tiles[1]].reshape(count * STRIP, width)
        gate_h = jnp.dot(rows_in, wg[...], preferred_element_type=f32)
        up_h = jnp.dot(rows_in, wu[...], preferred_element_type=f32)
        hidden = (gate_h * jax.nn.sigmoid(gate_h) * up_h).astype(bf16)
        fo[group, tiles[0] : tiles[1]] = (
            jnp.dot(hidden, wd[...], preferred_element_type=f32)
            .astype(bf16)
            .reshape(count, STRIP, width)
        )

    def give_part(group, tiles, cols, turn, no):
        return slots_copies(
            fo,
            rr,
            group,
            tiles,
            cols,
            lambda j: h_s.at[group, turn, no, j],
            lambda j: h_r.at[group, turn, no, j],
        )

    def combine(group, rows, tiles, cols):
        weights = jnp.where(hits(group, rows, tiles), table(group, 1, tiles), 0.0)
        high = weights.astype(bf16)
        low = (weights - high.astype(f32)).astype(bf16)
        at, size = cols
        back = rr[group, tiles[0] : tiles[1], :, pl.ds(aligned(at), size)]
        back = back.reshape((tiles[1] - tiles[0]) * STRIP, size)
        return jnp.dot(high, back, preferred_element_type=f32) + jnp.dot(
            low, back, preferred_element_type=f32
        )

    every, later, side_tiles = (0, TILES), (0, LATE), ((0, 2), (1, 3))

    def half_of(way, by):
        turned = (lax.rem(z + by + Z, Z) // 2) % 2
        return (turned if way == 0 else 1 - turned) * half

    def reduced_copy(way, hop, no):
        cols = pl.ds(no * share, share)
        return remote(
            rs.at[way, hop, pl.ds(0, tokens), cols],
            rv.at[way, hop, pl.ds(0, tokens), cols],
            rs_s.at[way, hop, no],
            rs_r.at[way, hop, no],
            ahead[way],
        )

    def side_rows(side):
        return (side * tokens, (side + 1) * tokens)

    def own_term(way, hop, no):
        distance = hop + 1
        owner = distance if way else -distance
        cols = (half_of(way, owner) + no * share, share)
        if distance == GROUPS:
            return combine(0, side_rows(1), later, cols)
        if distance < GROUPS:
            group, side = distance, way
        else:
            group, side = Z - distance, 1 - way
        return combine(group, side_rows(side), side_tiles[side], cols)

    def came(way, hop, no):
        return rv[way, hop, :, no * share : (no + 1) * share].astype(f32)

    def reduce_step(hop, coming, ready):
        passed = {}
        for no in range(2):
            finish(ready[no])
            for way in range(2):
                total = own_term(way, hop, no)
                if hop:
                    coming[way, no].wait_recv()
                    total = total + came(way, hop - 1, no)
                rs[way, hop, :, no * share : (no + 1) * share] = total.astype(bf16)
                passed[way, no] = begin(reduced_copy(way, hop, no))
        return passed

    def give_first(group):
        left = half_of(0, -group)
        copies = []
        for no in range(2):
            cols = (left + no * share, share)
            if group % 2:
                copies.append(give_part(group, every, cols, no, 0))
            else:
                other = (half - left + no * share, share)
                copies.append(
                    give_part(group, side_tiles[0], cols, no, 0)
                    + give_part(group, side_tiles[1], other, no, 1)
                )
        return copies

    def give_rest(group):
        left = half_of(0, -group)
        if group % 2:
            return give_part(group, every, (half - left, half), 2, 0)
        return give_part(group, (2, 3), (left, half), 2, 0) + give_part(
            group, (0, 1), (half - left, half), 2, 1
        )

    def give_late(no):
        copies = []
        for side in range(2):
            copies += slots_copies(
                fo,
                rr,
                0,
                later,
                (side * half + no * share, share),
                lambda j: b_s.at[no, side, j],
                lambda j: b_r.at[no, side, j],
            )
        return copies

    dealt, given, rest = {}, {}, {}
    for step in range(1, GROUPS):
        passed = {}
        dealt[step] = []
        farthest = step == GROUPS - 1
        for chunk in range(PARTS):
            for way in range(2):
                arriving[way, chunk].wait_recv()
                if farthest and chunk % 2 != way:
                    continue
                src = ag.at[step, pl.ds(way * tokens, tokens), pl.ds(chunk * share, share)]
                group, side = (0, 1) if farthest else (step + 1, way)
                passed[way, chunk] = begin(gather_copy(src, group, side, chunk, way, step))
            dealt[step] += dispatch(step, chunk, every)
            if chunk == 2 * step - 3 and step > 1:
                finish(dealt[step - 1])
                experts(step - 1, every)
                given[step - 1] = give_first(step - 1)
            if chunk == PARTS - 1 and step == 1:
                finish(early)
                experts(0, (LATE, TILES))
        arriving = passed
    coming = reduce_step(0, {}, given[1])
    dealt[0] = []
    for chunk in range(PARTS):
        arriving[chunk % 2, chunk].wait_recv()
        dealt[0] += dispatch(0, chunk, later)
    last = GROUPS - 1
    finish(dealt[last])
    experts(last, every)
    given[last] = give_first(last)
    coming = reduce_step(1, coming, given[2])
    finish(dealt[0])
    experts(0, later)
    given[0] = [give_late(no) for no in range(2)]
    for group in range(last, 0, -1):
        rest[group] = give_rest(group)
    given_early = slots_copies(
        fo, rr, 0, (LATE, TILES), whole, lambda j: l_s.at[j], lambda j: l_r.at[j]
    )
    coming = reduce_step(2, coming, given[last])
    coming = reduce_step(3, coming, given[0])
    for hop in range(GROUPS, HOPS):
        coming = reduce_step(hop, coming, (rest[HOPS - hop], ()))
    finish(given_early)
    acc[...] += combine(0, side_rows(0), every, whole)
    for no in range(2):
        for way in range(2):
            coming[way, no].wait_recv()
            cols = pl.ds(aligned(half_of(way, 0) + no * share), share)
            acc[:, cols] += came(way, HOPS - 1, no)

    branch = acc[...]
    factor = lax.rsqrt(jnp.mean(branch * branch, axis=1, keepdims=True) + epsilon)
    out[...] = (resid[...].astype(jnp.float32) + branch * factor * row_of(post_gain)).astype(
        jnp.bfloat16
    )
    for copy in started:
        copy.wait_send()


def body(
    x_in,
    gate_b,
    gate_c,
    conv_taps,
    out_proj,
    mix_gain,
    resid,
    pre_gain,
    expert_gate,
    expert_up,
    expert_down,
    shared_gate,
    shared_up,
    shared_down,
    post_gain,
    routes,
    route_weights,
):
    tokens, width = resid.shape
    rows, channels = x_in.shape
    hidden = expert_gate.shape[2]
    shared = shared_gate.shape[1]
    bf16, f32 = jnp.bfloat16, jnp.float32
    vmem = pl.BlockSpec(memory_space=pltpu.VMEM)
    hbm = pl.BlockSpec(memory_space=pl.ANY)
    dma = pltpu.SemaphoreType.DMA
    return pl.pallas_call(
        layer_kernel,
        out_shape=pltpu.VMEM((tokens, width), bf16),
        in_specs=[hbm] * 17,
        out_specs=vmem,
        scratch_shapes=[
            pltpu.VMEM(conv_taps.shape, bf16),
            pltpu.VMEM((width // 128, 128), bf16),
            pltpu.VMEM((width // 128, 128), bf16),
            pltpu.VMEM((width // 128, 128), bf16),
            pltpu.VMEM(routes.shape[::-1], jnp.int32),
            pltpu.VMEM(route_weights.shape[::-1], f32),
            pltpu.VMEM((rows, channels), bf16),
            pltpu.VMEM((rows, channels), bf16),
            pltpu.VMEM((rows, channels), bf16),
            pltpu.VMEM((2, 8, channels), bf16),
            pltpu.VMEM((rows + 8, channels), f32),
            pltpu.VMEM((rows, channels), bf16),
            pltpu.VMEM((Y, tokens, channels), bf16),
            pltpu.VMEM((Y, channels, width), bf16),
            pltpu.VMEM((tokens, width), bf16),
            pltpu.VMEM((tokens, width), bf16),
            pltpu.VMEM((GROUPS, 2 * tokens, width), bf16),
            pltpu.VMEM((Z, 8, META), f32),
            pltpu.VMEM((Z, 8, META), f32),
            pltpu.VMEM((GROUPS, TILES, STRIP, width), bf16),
            pltpu.VMEM((GROUPS, TILES, STRIP, width), bf16),
            pltpu.VMEM((GROUPS, TILES, STRIP, width), bf16),
            pltpu.VMEM((GROUPS, TILES, STRIP, width), bf16),
            pltpu.VMEM((tokens, width), f32),
            pltpu.VMEM((2, HOPS, tokens, width // 2), bf16),
            pltpu.VMEM((2, HOPS, tokens, width // 2), bf16),
            pltpu.VMEM((tokens, width), f32),
            pltpu.VMEM((width, hidden), bf16),
            pltpu.VMEM((width, hidden), bf16),
            pltpu.VMEM((hidden, width), bf16),
            pltpu.VMEM((width, shared), bf16),
            pltpu.VMEM((width, shared), bf16),
            pltpu.VMEM((shared, width), bf16),
            dma((17,)),
            dma((2,)),
            dma((2,)),
            dma((2,)),
            dma((Y,)),
            dma((Y,)),
            dma((Y, SUBS)),
            dma((Y, SUBS)),
            dma((Y, SUBS)),
            dma((Y, SUBS)),
            dma((Y, 2, SUBS)),
            dma((Y, 2, SUBS)),
            dma((2, GROUPS, PARTS)),
            dma((2, GROUPS, PARTS)),
            dma((Z,)),
            dma((Z,)),
            dma((GROUPS, PARTS, PLANE)),
            dma((GROUPS, PARTS, PLANE)),
            dma((PLANE,)),
            dma((PLANE,)),
            dma((2, 2, PLANE)),
            dma((2, 2, PLANE)),
            dma((PLANE,)),
            dma((PLANE,)),
            dma((GROUPS, 3, 2, PLANE)),
            dma((GROUPS, 3, 2, PLANE)),
            dma((2, HOPS, 2)),
            dma((2, HOPS, 2)),
        ],
        compiler_params=pltpu.CompilerParams(
            collective_id=0, has_side_effects=True, vmem_limit_bytes=63 * 1024 * 1024
        ),
    )(
        conv_taps,
        mix_gain.reshape(-1, 128),
        pre_gain.reshape(-1, 128),
        post_gain.reshape(-1, 128),
        routes.T,
        route_weights.T,
        x_in,
        gate_b,
        gate_c,
        out_proj,
        resid,
        expert_gate[0],
        expert_up[0],
        expert_down[0],
        shared_gate,
        shared_up,
        shared_down,
    )


def solution(mesh):
    finer = Mesh(mesh.devices.reshape(Z, X, C, mesh.shape["tp"]), SP_TP)
    placed = (
        P(SP, "tp"),
        P(SP, "tp"),
        P(SP, "tp"),
        P(None, "tp"),
        P("tp", None),
        P(),
        P(SP_TP, None),
        P(),
        P(SP, None, None),
        P(SP, None, None),
        P(SP, None, None),
        P(),
        P(),
        P(),
        P(),
        P(SP_TP, None),
        P(SP_TP, None),
    )
    return jax.shard_map(
        body, mesh=finer, in_specs=placed, out_specs=P(SP_TP, None), check_vma=False
    )
```
